32 devices in a mesh: sp: 4 (over z), fs: 4 (over y, x), tp: 2 (over core).
Axes of the slice: x: 2, y: 2, z: 4, core: 2. Of those that a mesh axis runs over, the one named last changes fastest.
Arguments:
- tokens: bfloat16 [4, 640, 2048], P('fs', 'sp', 'tp'), may hold values from -6 to 6
- mix_gain: float32 [2048], replicated, may hold values from 0.1 to 1.9
- conv_b_weight: bfloat16 [2048, 1024], P(('sp', 'fs'), 'tp'), may hold values from -0.125 to 0.125
- conv_c_weight: bfloat16 [2048, 1024], P(('sp', 'fs'), 'tp'), may hold values from -0.125 to 0.125
- conv_v_weight: bfloat16 [2048, 1024], P(('sp', 'fs'), 'tp'), may hold values from -0.125 to 0.125
- conv_taps: float32 [3, 1024], P(None, 'tp'), may hold values from -3.5 to 3.5
- query_weight: bfloat16 [2048, 2048], P(('sp', 'fs'), 'tp'), may hold values from -0.125 to 0.125
- query_rope_weight: bfloat16 [2048, 1024], P(('sp', 'fs'), 'tp'), may hold values from -4.5 to 4.5
- latent_weight: bfloat16 [2048, 512], P(('sp', 'fs')), may hold values from -0.125 to 0.125
- key_rope_weight: bfloat16 [2048, 64], replicated, may hold values from -1 to 1
- latent_gain: float32 [512], replicated, may hold values from 0.1 to 1.9
- key_up_weight: bfloat16 [512, 2048], P(None, 'tp'), may hold values from -0.25 to 0.25
- value_up_weight: bfloat16 [512, 2048], P(None, 'tp'), may hold values from -0.25 to 0.25
- head_gain: float32 [2048], P('tp'), may hold values from 0.1 to 1.9
- conv_out_weight: bfloat16 [1024, 2048], P('tp', ('sp', 'fs')), may hold values from -0.109375 to 0.109375
- attn_out_weight: bfloat16 [2048, 2048], P('tp', ('sp', 'fs')), may hold values from -0.109375 to 0.109375
Outputs:
- mixed: bfloat16 [4, 640, 2048], P('fs', ('sp', 'tp'))
The draws below stay inside these ranges and needn't reach their ends.
All inputs are finite; a program needn't handle non-finite values.
Results may differ from the reference program's by a relative error of at most 0.025.
Values may be sent and summed in bfloat16 or wider, within the bound.
No kernel may reach another device: no remote copies, remote signals or barrier semaphores. Data moves between devices by JAX's collectives and lax.ppermute only.
A program may use at most 128 MiB of HBM per device.

```python
import math
import jax
import jax.numpy as jnp
from jax import lax

D = 2048
CONV = 1024
H = 16
NOPE = 128
ROPE = 64
VD = 128
KVL = 512
SEG = 64
SEQS = 4
LENGTH = 640
N_TP = 2


def rope_base(key):
    base = jax.random.normal(jax.random.fold_in(key, 101), (D, ROPE), jnp.float32)
    return jnp.clip(base, -4.0, 4.0) * D ** (-0.5)


def draw_key_rope_weight(key, part):
    return rope_base(key).astype(jnp.bfloat16)


def draw_query_rope_weight(key, part):
    fresh = jax.random.normal(jax.random.fold_in(key, 102), (D, H, ROPE), jnp.float32)
    fresh = jnp.clip(fresh, -4.0, 4.0) * D ** (-0.5)
    shaped = fresh
    return shaped.reshape(D, H * ROPE).astype(jnp.bfloat16)


def block_levels(rng, dims, split, least, high):
    loudness = 1.0
    for dim, parts in split:
        heights = jax.random.uniform(jax.random.fold_in(jax.random.fold_in(rng, 6), dim), (parts,), jnp.float32, least / len(split), high / len(split))
        loudness = loudness * jnp.repeat(jnp.exp(heights), dims[dim] // parts).reshape((-1,) + (1,) * (len(dims) - 1 - dim))
    return loudness


def bell_draw(stream_key, dims, width, bound, shards=(), kind=jnp.bfloat16):
    values = width * jax.random.normal(stream_key, dims, jnp.float32)
    if shards:
        values = values * block_levels(stream_key, dims, shards, -0.22, 0.18)
    return jnp.clip(values, -bound, bound).astype(kind)


def setup_inputs(seed: int = 0) -> dict:
    seeds = jax.random.split(jax.random.key(seed), 17)
    return {
        "tokens": bell_draw(seeds[0], (SEQS, LENGTH, D), 1.0, 6.0, ((0, 4), (1, 4), (2, 2))),
        "mix_gain": jnp.clip(1.0 + 0.18 * jax.random.normal(seeds[1], (D,), jnp.float32), 0.1, 1.9),
        "conv_b_weight": bell_draw(seeds[2], (D, CONV), D ** -0.5, 0.125, ((0, 16), (1, 2))),
        "conv_c_weight": bell_draw(seeds[3], (D, CONV), D ** -0.5, 0.125, ((0, 16), (1, 2))),
        "conv_v_weight": bell_draw(seeds[4], (D, CONV), D ** -0.5, 0.125, ((0, 16), (1, 2))),
        "conv_taps": bell_draw(seeds[5], (3, CONV), 3 ** -0.5, 3.5, ((1, 2),), jnp.float32),
        "query_weight": bell_draw(seeds[6], (D, H * NOPE), D ** -0.5, 0.125, ((0, 16), (1, 2))),
        "query_rope_weight": draw_query_rope_weight(jax.random.fold_in(seeds[16], 71), 0),
        "latent_weight": bell_draw(seeds[8], (D, KVL), D ** -0.5, 0.125, ((0, 16),)),
        "key_rope_weight": draw_key_rope_weight(jax.random.fold_in(seeds[16], 71), 0),
        "latent_gain": jnp.clip(1.0 + 0.18 * jax.random.normal(seeds[10], (KVL,), jnp.float32), 0.1, 1.9),
        "key_up_weight": bell_draw(seeds[11], (KVL, H * NOPE), KVL ** -0.5, 0.25, ((1, 2),)),
        "value_up_weight": bell_draw(seeds[12], (KVL, H * VD), KVL ** -0.5, 0.25, ((1, 2),)),
        "head_gain": jnp.clip(1.0 + 0.18 * jax.random.normal(seeds[13], (H * VD,), jnp.float32), 0.1, 1.9),
        "conv_out_weight": bell_draw(seeds[14], (CONV, D), (CONV + H * VD) ** -0.5, 0.109375, ((0, 2), (1, 16))),
        "attn_out_weight": bell_draw(seeds[15], (H * VD, D), (CONV + H * VD) ** -0.5, 0.109375, ((0, 2), (1, 16))),
    }


norm_epsilon = 1e-06
rope_theta = 10000.0

def rms_scale(values, gain):
    return values * lax.rsqrt(lax.optimization_barrier(jnp.mean(values * values, axis=-1, keepdims=True)) + norm_epsilon) * gain

def rope_tables(positions):
    half_width = ROPE // 2
    frequency = rope_theta ** (-jnp.arange(half_width, dtype=jnp.float32) * 2.0 / ROPE)
    angles = positions[:, None] * frequency[None, :]
    return (jnp.cos(angles), jnp.sin(angles))

def rotate(values, cosine, sine):
    half_width = ROPE // 2
    first = values[..., :half_width]
    second = values[..., half_width:]
    return jnp.concatenate([first * cosine - second * sine, second * cosine + first * sine], axis=-1)

def matmul(left, right):
    return jnp.dot(left, right, preferred_element_type=jnp.float32)

def one_sequence(sequence, mix_gain, conv_b_weight, conv_c_weight, conv_v_weight, conv_taps, query_weight, query_rope_weight, latent_weight, key_rope_weight, latent_gain, key_up_weight, value_up_weight, head_gain, conv_out_weight, attn_out_weight):
    length = sequence.shape[0]
    normed = rms_scale(sequence.astype(jnp.float32), mix_gain).astype(jnp.bfloat16)
    gate_b = matmul(normed, conv_b_weight).astype(jnp.bfloat16)
    gate_c = matmul(normed, conv_c_weight).astype(jnp.bfloat16)
    values_v = matmul(normed, conv_v_weight).astype(jnp.bfloat16)
    product = (gate_c.astype(jnp.float32) * values_v.astype(jnp.float32)).astype(jnp.bfloat16)
    padded = jnp.concatenate([jnp.zeros((2, CONV), jnp.bfloat16), product], axis=0).astype(jnp.float32)
    convolved = conv_taps[0] * padded[0:length] + conv_taps[1] * padded[1:length + 1] + conv_taps[2] * padded[2:length + 2]
    conv_y = (gate_b.astype(jnp.float32) * convolved).astype(jnp.bfloat16)
    positions = jnp.arange(length, dtype=jnp.float32)
    cosine, sine = rope_tables(positions)
    query_nope = matmul(normed, query_weight).astype(jnp.bfloat16).reshape(length, H, NOPE)
    query_rot = rotate(matmul(normed, query_rope_weight).reshape(length, H, ROPE), cosine[:, None, :], sine[:, None, :]).astype(jnp.bfloat16)
    latent_raw = matmul(normed, latent_weight).astype(jnp.bfloat16)
    latent = rms_scale(latent_raw.astype(jnp.float32), latent_gain).astype(jnp.bfloat16)
    key_rot = rotate(matmul(normed, key_rope_weight), cosine, sine).astype(jnp.bfloat16)
    query_latent = jnp.einsum('thn,khn->thk', query_nope.astype(jnp.float32), key_up_weight.reshape(KVL, H, NOPE).astype(jnp.float32)).astype(jnp.bfloat16)
    attn_scale = (NOPE + ROPE) ** (-0.5)
    block_rows = math.gcd(length, 512)
    latent_wide = latent.astype(jnp.float32)
    key_wide = key_rot.astype(jnp.float32)
    key_segment = jnp.arange(length, dtype=jnp.int32) // SEG

    def attend(block_index):
        begin_row = (block_index * block_rows).astype(jnp.int32)
        block_latent = lax.dynamic_slice_in_dim(query_latent, begin_row, block_rows, 0).astype(jnp.float32)
        block_rot = lax.dynamic_slice_in_dim(query_rot, begin_row, block_rows, 0).astype(jnp.float32)
        scores = (jnp.einsum('thk,jk->thj', block_latent, latent_wide) + jnp.einsum('thr,jr->thj', block_rot, key_wide)) * attn_scale
        query_segment = (begin_row + jnp.arange(block_rows, dtype=jnp.int32)) // SEG
        allowed = key_segment[None, None, :] <= query_segment[:, None, None]
        scores = jnp.where(allowed, scores, -1e+30)
        highest = lax.optimization_barrier(jnp.max(scores, axis=-1, keepdims=True))
        weights = jnp.where(allowed, jnp.exp(scores - highest), 0.0)
        summed = lax.optimization_barrier(jnp.sum(weights, axis=-1))
        numer = jnp.einsum('thj,jk->thk', weights.astype(jnp.bfloat16).astype(jnp.float32), latent_wide)
        return (numer / summed[..., None]).astype(jnp.bfloat16)
    attended = lax.map(attend, jnp.arange(length // block_rows, dtype=jnp.int32)).reshape(length, H, KVL)
    head_out = jnp.einsum('thk,khv->thv', attended.astype(jnp.float32), value_up_weight.reshape(KVL, H, VD).astype(jnp.float32))
    attn_y = rms_scale(head_out, head_gain.reshape(H, VD)).astype(jnp.bfloat16).reshape(length, H * VD)
    conv_share = CONV // N_TP
    head_share = H * VD // N_TP
    combined = jnp.zeros((length, D), jnp.float32)
    for share in range(N_TP):
        conv_cols = slice(share * conv_share, (share + 1) * conv_share)
        head_cols = slice(share * head_share, (share + 1) * head_share)
        partial_out = matmul(conv_y[:, conv_cols], conv_out_weight[conv_cols]) + matmul(attn_y[:, head_cols], attn_out_weight[head_cols])
        rounded = lax.optimization_barrier(partial_out.astype(jnp.bfloat16))
        combined = combined + rounded.astype(jnp.float32)
    return combined.astype(jnp.bfloat16)

def reference(tokens, mix_gain, conv_b_weight, conv_c_weight, conv_v_weight, conv_taps, query_weight, query_rope_weight, latent_weight, key_rope_weight, latent_gain, key_up_weight, value_up_weight, head_gain, conv_out_weight, attn_out_weight):
    results = []
    for sequence_index in range(SEQS):
        results.append(one_sequence(tokens[sequence_index], mix_gain, conv_b_weight, conv_c_weight, conv_v_weight, conv_taps, query_weight, query_rope_weight, latent_weight, key_rope_weight, latent_gain, key_up_weight, value_up_weight, head_gain, conv_out_weight, attn_out_weight))
    return jnp.stack(results, axis=0)
```

```python
import jax
import jax.numpy as jnp
from jax import lax
from jax.sharding import PartitionSpec as P

NOPE = 128
ROPE = 64
VD = 128
KVL = 512
SEG = 64


norm_epsilon = 1e-06
rope_theta = 10000.0


def passed_along(block, axis, distance):
    devices = range(lax.axis_size(axis))
    route = [(i - distance, i) for i in devices if i - distance in devices]
    return lax.ppermute(block, axis, route)


def rms_scale(values, gain):
    return (
        values * lax.rsqrt(jnp.mean(values * values, axis=-1, keepdims=True) + norm_epsilon) * gain
    )


def rope_tables(positions):
    half_width = ROPE // 2
    frequency = rope_theta ** (-jnp.arange(half_width, dtype=jnp.float32) * 2.0 / ROPE)
    angles = positions[:, None] * frequency[None, :]
    return (jnp.cos(angles), jnp.sin(angles))


def rotate(values, cosine, sine):
    half_width = ROPE // 2
    first = values[..., :half_width]
    second = values[..., half_width:]
    return jnp.concatenate(
        [first * cosine - second * sine, second * cosine + first * sine], axis=-1
    )


def token_parallel(
    tokens,
    mix_gain,
    conv_b_weight,
    conv_c_weight,
    conv_v_weight,
    conv_taps,
    query_weight,
    query_rope_weight,
    latent_weight,
    key_rope_weight,
    latent_gain,
    key_up_weight,
    value_up_weight,
    head_gain,
    conv_out_weight,
    attn_out_weight,
):
    full_rows = lax.all_gather(tokens[0], "tp", axis=1, tiled=True)
    tok_rows = full_rows.shape[0]
    normed = rms_scale(full_rows.astype(jnp.float32), mix_gain).astype(jnp.bfloat16)
    offset = lax.axis_index("sp") * tok_rows
    token_index = offset + jnp.arange(tok_rows, dtype=jnp.int32)
    cosine, sine = rope_tables(token_index.astype(jnp.float32))
    local_heads = query_weight.shape[1] // NOPE
    count_sp = lax.axis_size("sp")
    count_fs = lax.axis_size("fs")
    count_tp = lax.axis_size("tp")
    fs_index = lax.axis_index("fs")
    row_piece = normed.shape[1] // (count_sp * count_fs)
    all_normed = lax.all_gather(normed, "fs", axis=0, tiled=True)
    picked = lax.dynamic_index_in_dim(
        all_normed.reshape(-1, count_sp, count_fs, row_piece), fs_index, 2, keepdims=False
    ).reshape(-1, count_sp * row_piece)
    gathered = (
        lax.all_gather(conv_b_weight, "sp", axis=0, tiled=True),
        lax.all_gather(conv_c_weight, "sp", axis=0, tiled=True),
        lax.all_gather(conv_v_weight, "sp", axis=0, tiled=True),
        lax.all_gather(query_weight, "sp", axis=0, tiled=True),
        lax.all_gather(query_rope_weight, "sp", axis=0, tiled=True),
        lax.all_gather(latent_weight, "sp", axis=0, tiled=True),
    )

    def project_in():
        return jnp.concatenate(
            [jnp.dot(picked, member, preferred_element_type=jnp.float32) for member in gathered],
            axis=1,
        )

    joined = lax.psum_scatter(
        project_in().astype(jnp.bfloat16), "fs", scatter_dimension=0, tiled=True
    ).astype(jnp.float32)
    bounds = []
    running_total = 0
    for member in gathered[:-1]:
        running_total = running_total + member.shape[1]
        bounds.append(running_total)
    sums = tuple(jnp.split(joined, bounds, axis=1))
    latent_raw = sums[5].astype(jnp.bfloat16)
    gate_b = sums[0].astype(jnp.bfloat16)
    gate_c = sums[1].astype(jnp.bfloat16)
    values_v = sums[2].astype(jnp.bfloat16)
    query_nope = sums[3].astype(jnp.bfloat16).reshape(tok_rows, local_heads, NOPE)
    query_rot = rotate(
        sums[4].reshape(tok_rows, local_heads, ROPE), cosine[:, None, :], sine[:, None, :]
    ).astype(jnp.bfloat16)
    latent = rms_scale(latent_raw.astype(jnp.float32), latent_gain).astype(jnp.bfloat16)
    key_rot = rotate(
        jnp.dot(normed, key_rope_weight, preferred_element_type=jnp.float32), cosine, sine
    ).astype(jnp.bfloat16)
    query_latent = jnp.einsum(
        "thn,khn->thk",
        query_nope,
        key_up_weight.reshape(KVL, local_heads, NOPE),
        preferred_element_type=jnp.float32,
    ).astype(jnp.bfloat16)
    attn_scale = (NOPE + ROPE) ** (-0.5)
    product = (gate_c.astype(jnp.float32) * values_v.astype(jnp.float32)).astype(jnp.bfloat16)
    previous = passed_along(product[tok_rows - 2 :], "sp", 1)
    padded = jnp.concatenate([previous, product], axis=0).astype(jnp.float32)
    convolved = (
        conv_taps[0] * padded[0:tok_rows]
        + conv_taps[1] * padded[1 : tok_rows + 1]
        + conv_taps[2] * padded[2 : tok_rows + 2]
    )
    conv_y = (gate_b.astype(jnp.float32) * convolved).astype(jnp.bfloat16)
    query_segment = token_index // SEG
    last_segment = (offset + tok_rows - 1) // SEG

    def key_block(running, latent_block, rot_block, first_key):
        peak_old, denom_old, accum_old = running
        block_rows = latent_block.shape[0]
        scores = (
            jnp.einsum(
                "thk,jk->thj", query_latent, latent_block, preferred_element_type=jnp.float32
            )
            + jnp.einsum("thr,jr->thj", query_rot, rot_block, preferred_element_type=jnp.float32)
        ) * attn_scale
        key_segment = (first_key + jnp.arange(block_rows, dtype=jnp.int32)) // SEG
        allowed = key_segment[None, None, :] <= query_segment[:, None, None]
        peak_new = jnp.maximum(peak_old, jnp.max(jnp.where(allowed, scores, -1e30), axis=-1))
        weights = jnp.where(allowed, jnp.exp(scores - peak_new[..., None]), 0.0)
        rescale = jnp.exp(peak_old - peak_new)
        denom_new = denom_old * rescale + jnp.sum(weights, axis=-1)
        accum_new = accum_old * rescale[..., None] + jnp.einsum(
            "thj,jk->thk",
            weights.astype(jnp.bfloat16),
            latent_block,
            preferred_element_type=jnp.float32,
        )
        return (peak_new, denom_new, accum_new)

    starting = (
        jnp.full((tok_rows, local_heads), -1e30, jnp.float32),
        jnp.zeros((tok_rows, local_heads), jnp.float32),
        jnp.zeros((tok_rows, local_heads, KVL), jnp.float32),
    )
    latent_piece = lax.all_gather(latent, "sp", axis=0, tiled=True)
    rot_piece = lax.all_gather(key_rot, "sp", axis=0, tiled=True)
    piece_rows = latent_piece.shape[0]
    splits = max(1, piece_rows // 512)
    while piece_rows % splits:
        splits = splits - 1
    block_rows = piece_rows // splits

    def visit(state, block_index):
        block_begin = block_index * block_rows
        latent_block = lax.dynamic_slice_in_dim(latent_piece, block_begin, block_rows, 0)
        rot_block = lax.dynamic_slice_in_dim(rot_piece, block_begin, block_rows, 0)
        updated = lax.cond(
            block_begin // SEG <= last_segment,
            lambda inner: key_block(inner, latent_block, rot_block, block_begin),
            lambda inner: inner,
            state,
        )
        return (updated, None)

    peak, denom, accum = lax.scan(visit, starting, jnp.arange(splits, dtype=jnp.int32))[0]
    attended = (accum / denom[..., None]).astype(jnp.bfloat16)
    head_out = jnp.einsum(
        "thk,khv->thv",
        attended,
        value_up_weight.reshape(KVL, local_heads, VD),
        preferred_element_type=jnp.float32,
    )
    normed_heads = rms_scale(head_out, head_gain.reshape(local_heads, VD))
    attn_y = normed_heads.astype(jnp.bfloat16).reshape(tok_rows, local_heads * VD)
    share_rows = tok_rows // count_tp
    conv_all, attn_all = (
        lax.all_gather(conv_y, "fs", axis=0, tiled=True),
        lax.all_gather(attn_y, "fs", axis=0, tiled=True),
    )
    conv_sorted = (
        conv_all.reshape(count_fs, count_tp, share_rows, -1)
        .transpose(1, 0, 2, 3)
        .reshape(count_fs * tok_rows, -1)
    )
    attn_sorted = (
        attn_all.reshape(count_fs, count_tp, share_rows, -1)
        .transpose(1, 0, 2, 3)
        .reshape(count_fs * tok_rows, -1)
    )
    conv_cols_sp, attn_cols_sp = (
        lax.all_gather(conv_out_weight, "sp", axis=1, tiled=True),
        lax.all_gather(attn_out_weight, "sp", axis=1, tiled=True),
    )
    col_sums = lax.psum_scatter(
        (
            jnp.dot(conv_sorted, conv_cols_sp, preferred_element_type=jnp.float32)
            + jnp.dot(attn_sorted, attn_cols_sp, preferred_element_type=jnp.float32)
        ).astype(jnp.bfloat16),
        "tp",
        scatter_dimension=0,
        tiled=True,
    )
    col_piece = conv_cols_sp.shape[1] // count_sp
    outgoing = col_sums.reshape(count_fs, share_rows, count_sp * col_piece)
    arrived = lax.all_to_all(outgoing, "fs", split_axis=0, concat_axis=2, tiled=True)
    result = (
        arrived.reshape(share_rows, count_fs, count_sp, col_piece)
        .transpose(0, 2, 1, 3)
        .reshape(share_rows, count_fs * count_sp * col_piece)
    )
    return result[None]


def turned(block, axis, distance):
    count = lax.axis_size(axis)
    return lax.ppermute(block, axis, [(i, (i + distance) % count) for i in range(count)])


def swapped(block, axis, mask):
    return lax.ppermute(block, axis, [(i, i ^ mask) for i in range(lax.axis_size(axis))])


def after(values, *others):
    return lax.optimization_barrier((values,) + others)[0]


def in_order(blocks, index):
    count = len(blocks)
    stacked = jnp.zeros((count,) + blocks[0].shape, blocks[0].dtype)
    for distance, block in enumerate(blocks):
        stacked = lax.dynamic_update_index_in_dim(
            stacked, block, (index - distance) % count, 0
        )
    return stacked


def exchange(packed, axis):
    count = lax.axis_size(axis)
    index = lax.axis_index(axis)
    blocks = [lax.dynamic_index_in_dim(packed, index, 0, keepdims=False)]
    for distance in range(1, count):
        outgoing = lax.dynamic_index_in_dim(packed, (index + distance) % count, 0, keepdims=False)
        blocks.append(turned(outgoing, axis, distance))
    return in_order(blocks, index)


def spread(block):
    by_one = swapped(block, "fs", 1)
    by_two = swapped(block, "fs", 2)
    half = block.shape[0] // 2
    upper = swapped(by_one[:half], "fs", 2)
    lower = swapped(by_two[half:], "fs", 1)
    return [block, by_one, by_two, jnp.concatenate([upper, lower], axis=0)]


def head_parallel(
    tokens,
    mix_gain,
    conv_b_weight,
    conv_c_weight,
    conv_v_weight,
    conv_taps,
    query_weight,
    query_rope_weight,
    latent_weight,
    key_rope_weight,
    latent_gain,
    key_up_weight,
    value_up_weight,
    head_gain,
    conv_out_weight,
    attn_out_weight,
):
    count_sp = lax.axis_size("sp")
    count_fs = lax.axis_size("fs")
    count_tp = lax.axis_size("tp")
    sp_index = lax.axis_index("sp")
    fs_index = lax.axis_index("fs")
    tp_index = lax.axis_index("tp")
    bf16 = jnp.bfloat16
    f32 = jnp.float32
    tok_rows = tokens.shape[1]
    length = tok_rows * count_sp
    row_piece = query_weight.shape[0]
    heads = query_weight.shape[1] // NOPE // count_sp
    chans = conv_b_weight.shape[1] // count_sp
    lat_half = latent_weight.shape[1] // count_tp
    lat_cols = lat_half // count_sp

    def by_target(weight):
        rows = weight.shape[0]
        return weight.reshape(rows, count_sp, -1).transpose(1, 0, 2)

    own_latent = lax.dynamic_slice_in_dim(latent_weight, tp_index * lat_half, lat_half, 1)
    pack_attn = jnp.concatenate(
        [by_target(w) for w in (query_weight, query_rope_weight, own_latent)], axis=2
    )
    pack_conv = jnp.concatenate(
        [by_target(w) for w in (conv_b_weight, conv_c_weight, conv_v_weight)], axis=2
    )
    arrived_attn = exchange(pack_attn, "sp")
    parts_attn = spread(arrived_attn)

    pack_conv = after(pack_conv, arrived_attn)
    arrived_conv = exchange(pack_conv, "sp")

    own = tokens[0]
    own_token = own
    halves = [own]
    for distance in range(1, count_sp):
        halves.append(turned(own_token, "sp", distance))
    normed_blocks = []
    for half in halves:
        other = swapped(half, "tp", 1)
        wide = jnp.where(
            tp_index == 0,
            jnp.concatenate([half, other], axis=1),
            jnp.concatenate([other, half], axis=1),
        )
        normed_blocks.append(rms_scale(wide.astype(f32), mix_gain).astype(bf16))
    normed = in_order(normed_blocks, sp_index).reshape(length, -1)

    split = normed.reshape(length, count_sp, count_fs, row_piece)
    facing = [
        lax.dynamic_index_in_dim(split, fs_index ^ m, 2, keepdims=False).reshape(length, -1)
        for m in range(count_fs)
    ]

    def project(parts):
        total = 0.0
        for columns, part in zip(facing, parts):
            total = total + jnp.dot(
                columns, part.reshape(count_sp * row_piece, -1), preferred_element_type=f32
            )
        return total

    arrived_conv = after(arrived_conv, *parts_attn)
    parts_conv = spread(arrived_conv)

    attn_in = project(parts_attn)
    edge_rot = heads * NOPE
    edge_lat = edge_rot + heads * ROPE
    latent_cols = attn_in[:, edge_lat:].astype(bf16)
    lat_blocks = [latent_cols] + [turned(latent_cols, "sp", d) for d in range(1, count_sp)]
    lat_mine = in_order(lat_blocks, sp_index).transpose(1, 0, 2).reshape(length, lat_half)
    lat_other = swapped(lat_mine, "tp", 1)
    latent_raw = jnp.where(
        tp_index == 0,
        jnp.concatenate([lat_mine, lat_other], axis=1),
        jnp.concatenate([lat_other, lat_mine], axis=1),
    )
    latent = rms_scale(latent_raw.astype(f32), latent_gain).astype(bf16)

    position = jnp.arange(length, dtype=jnp.int32)
    cosine, sine = rope_tables(position.astype(f32))
    key_rot = rotate(
        jnp.dot(normed, key_rope_weight, preferred_element_type=f32), cosine, sine
    ).astype(bf16)
    query_nope = attn_in[:, :edge_rot].astype(bf16).reshape(length, heads, NOPE)
    query_rot = rotate(
        attn_in[:, edge_rot:edge_lat].reshape(length, heads, ROPE),
        cosine[:, None, :],
        sine[:, None, :],
    ).astype(bf16)

    def own_heads(weight, width):
        return lax.dynamic_slice_in_dim(
            weight, sp_index * heads * width, heads * width, weight.ndim - 1
        )

    key_up = own_heads(key_up_weight, NOPE).reshape(KVL, heads, NOPE)
    value_up = own_heads(value_up_weight, VD).reshape(KVL, heads, VD)
    gain = own_heads(head_gain, VD).reshape(heads, VD)
    taps = lax.dynamic_slice_in_dim(conv_taps, sp_index * chans, chans, 1)
    query_latent = jnp.einsum(
        "thn,khn->htk", query_nope, key_up, preferred_element_type=f32
    ).astype(bf16)

    pack_out = jnp.concatenate(
        [
            conv_out_weight.reshape(count_sp, chans, -1),
            attn_out_weight.reshape(count_sp, heads * VD, -1),
        ],
        axis=1,
    )
    pack_out = after(pack_out, *halves, arrived_conv)
    arrived_out = exchange(pack_out, "sp")
    arrived_out = after(arrived_out, *parts_conv)
    parts_out = spread(arrived_out)
    col_piece = conv_out_weight.shape[1]
    out_stack = jnp.zeros((count_fs,) + arrived_out.shape, bf16)
    for m in range(count_fs):
        out_stack = lax.dynamic_update_index_in_dim(out_stack, parts_out[m], fs_index ^ m, 0)
    out_weight = out_stack.transpose(2, 1, 0, 3).reshape(
        arrived_out.shape[1], count_sp * count_fs * col_piece
    )

    conv_in = project(parts_conv).astype(bf16).astype(f32)
    gate_b = conv_in[:, :chans]
    product = (conv_in[:, chans : 2 * chans] * conv_in[:, 2 * chans :]).astype(bf16)
    padded = jnp.concatenate([jnp.zeros((2, chans), bf16), product], axis=0).astype(f32)
    convolved = (
        taps[0] * padded[0:length] + taps[1] * padded[1 : length + 1] + taps[2] * padded[2:]
    )
    conv_y = (gate_b * convolved).astype(bf16)

    attn_scale = (NOPE + ROPE) ** (-0.5)
    queries = jnp.concatenate([query_latent, query_rot.transpose(1, 0, 2)], axis=2)
    keys = jnp.concatenate([latent, key_rot], axis=1)
    scores = jnp.einsum("htk,jk->htj", queries, keys, preferred_element_type=f32) * attn_scale
    segment = position // SEG
    allowed = (segment[None, :] <= segment[:, None])[None]
    scores = jnp.where(allowed, scores, -1e30)
    top = jnp.max(scores, axis=-1, keepdims=True)
    weights = jnp.where(allowed, jnp.exp(scores - top), 0.0)
    total = jnp.sum(weights, axis=-1, keepdims=True)
    accum = jnp.einsum(
        "htj,jk->htk", weights.astype(bf16), latent, preferred_element_type=f32
    )
    attended = (accum / total).astype(bf16)
    head_out = jnp.einsum("htk,khv->thv", attended, value_up, preferred_element_type=f32)
    attn_y = rms_scale(head_out, gain).astype(bf16).reshape(length, heads * VD)
    mixers = jnp.concatenate([conv_y, attn_y], axis=1).reshape(count_sp, tok_rows, -1)

    share = tok_rows // count_tp
    final = None
    for distance in [*range(count_sp - 1, 0, -1), 0]:
        target = (sp_index + distance) % count_sp
        rows = lax.dynamic_index_in_dim(mixers, target, 0, keepdims=False)
        partial = jnp.dot(rows, out_weight, preferred_element_type=f32).astype(bf16)
        partial = partial.reshape(count_tp, share, -1)
        keep = lax.dynamic_index_in_dim(partial, tp_index, 0, keepdims=False)
        give = lax.dynamic_index_in_dim(partial, 1 - tp_index, 0, keepdims=False)
        both = keep.astype(f32) + swapped(give, "tp", 1).astype(f32)
        if distance:
            both = turned(both.astype(bf16), "sp", distance).astype(f32)
        final = both if final is None else final + both
    return final.astype(bf16)[None]


def solution(mesh):
    sizes = dict(mesh.shape)
    divided = sizes["sp"] * sizes["tp"]
    fits = sizes["tp"] == 2 and sizes["fs"] == 4

    def shards(*args):
        heads = args[6].shape[1] // NOPE
        chans = args[2].shape[1]
        even = heads % sizes["sp"] == 0 and chans % sizes["sp"] == 0 and KVL % divided == 0
        if fits and even:
            return head_parallel(*args)
        return token_parallel(*args)

    return jax.shard_map(
        shards,
        mesh=mesh,
        in_specs=(
            P("fs", "sp", "tp"),
            P(),
            P(("sp", "fs"), "tp"),
            P(("sp", "fs"), "tp"),
            P(("sp", "fs"), "tp"),
            P(None, "tp"),
            P(("sp", "fs"), "tp"),
            P(("sp", "fs"), "tp"),
            P(("sp", "fs"), None),
            P(),
            P(),
            P(None, "tp"),
            P(None, "tp"),
            P("tp"),
            P("tp", ("sp", "fs")),
            P("tp", ("sp", "fs")),
        ),
        out_specs=P("fs", ("sp", "tp"), None),
        check_vma=False,
    )
```

```python
import jax
import jax.numpy as jnp
from jax import lax
from jax.experimental import pallas as pl
from jax.experimental.pallas import tpu as pltpu
from jax.sharding import PartitionSpec as P

NOPE = 128
ROPE = 64
VD = 128
KVL = 512
SEG = 64


norm_epsilon = 1e-06
rope_theta = 10000.0


def passed_along(block, axis, distance):
    devices = range(lax.axis_size(axis))
    route = [(i - distance, i) for i in devices if i - distance in devices]
    return lax.ppermute(block, axis, route)


def rms_scale(values, gain):
    return (
        values * lax.rsqrt(jnp.mean(values * values, axis=-1, keepdims=True) + norm_epsilon) * gain
    )


def rope_tables(positions):
    half_width = ROPE // 2
    frequency = rope_theta ** (-jnp.arange(half_width, dtype=jnp.float32) * 2.0 / ROPE)
    angles = positions[:, None] * frequency[None, :]
    return (jnp.cos(angles), jnp.sin(angles))


def rotate(values, cosine, sine):
    half_width = ROPE // 2
    first = values[..., :half_width]
    second = values[..., half_width:]
    return jnp.concatenate(
        [first * cosine - second * sine, second * cosine + first * sine], axis=-1
    )


def token_parallel(
    tokens,
    mix_gain,
    conv_b_weight,
    conv_c_weight,
    conv_v_weight,
    conv_taps,
    query_weight,
    query_rope_weight,
    latent_weight,
    key_rope_weight,
    latent_gain,
    key_up_weight,
    value_up_weight,
    head_gain,
    conv_out_weight,
    attn_out_weight,
):
    full_rows = lax.all_gather(tokens[0], "tp", axis=1, tiled=True)
    tok_rows = full_rows.shape[0]
    normed = rms_scale(full_rows.astype(jnp.float32), mix_gain).astype(jnp.bfloat16)
    offset = lax.axis_index("sp") * tok_rows
    token_index = offset + jnp.arange(tok_rows, dtype=jnp.int32)
    cosine, sine = rope_tables(token_index.astype(jnp.float32))
    local_heads = query_weight.shape[1] // NOPE
    count_sp = lax.axis_size("sp")
    count_fs = lax.axis_size("fs")
    count_tp = lax.axis_size("tp")
    fs_index = lax.axis_index("fs")
    row_piece = normed.shape[1] // (count_sp * count_fs)
    all_normed = lax.all_gather(normed, "fs", axis=0, tiled=True)
    picked = lax.dynamic_index_in_dim(
        all_normed.reshape(-1, count_sp, count_fs, row_piece), fs_index, 2, keepdims=False
    ).reshape(-1, count_sp * row_piece)
    gathered = (
        lax.all_gather(conv_b_weight, "sp", axis=0, tiled=True),
        lax.all_gather(conv_c_weight, "sp", axis=0, tiled=True),
        lax.all_gather(conv_v_weight, "sp", axis=0, tiled=True),
        lax.all_gather(query_weight, "sp", axis=0, tiled=True),
        lax.all_gather(query_rope_weight, "sp", axis=0, tiled=True),
        lax.all_gather(latent_weight, "sp", axis=0, tiled=True),
    )

    def project_in():
        return jnp.concatenate(
            [jnp.dot(picked, member, preferred_element_type=jnp.float32) for member in gathered],
            axis=1,
        )

    joined = lax.psum_scatter(
        project_in().astype(jnp.bfloat16), "fs", scatter_dimension=0, tiled=True
    ).astype(jnp.float32)
    bounds = []
    running_total = 0
    for member in gathered[:-1]:
        running_total = running_total + member.shape[1]
        bounds.append(running_total)
    sums = tuple(jnp.split(joined, bounds, axis=1))
    latent_raw = sums[5].astype(jnp.bfloat16)
    gate_b = sums[0].astype(jnp.bfloat16)
    gate_c = sums[1].astype(jnp.bfloat16)
    values_v = sums[2].astype(jnp.bfloat16)
    query_nope = sums[3].astype(jnp.bfloat16).reshape(tok_rows, local_heads, NOPE)
    query_rot = rotate(
        sums[4].reshape(tok_rows, local_heads, ROPE), cosine[:, None, :], sine[:, None, :]
    ).astype(jnp.bfloat16)
    latent = rms_scale(latent_raw.astype(jnp.float32), latent_gain).astype(jnp.bfloat16)
    key_rot = rotate(
        jnp.dot(normed, key_rope_weight, preferred_element_type=jnp.float32), cosine, sine
    ).astype(jnp.bfloat16)
    query_latent = jnp.einsum(
        "thn,khn->thk",
        query_nope,
        key_up_weight.reshape(KVL, local_heads, NOPE),
        preferred_element_type=jnp.float32,
    ).astype(jnp.bfloat16)
    attn_scale = (NOPE + ROPE) ** (-0.5)
    product = (gate_c.astype(jnp.float32) * values_v.astype(jnp.float32)).astype(jnp.bfloat16)
    previous = passed_along(product[tok_rows - 2 :], "sp", 1)
    padded = jnp.concatenate([previous, product], axis=0).astype(jnp.float32)
    convolved = (
        conv_taps[0] * padded[0:tok_rows]
        + conv_taps[1] * padded[1 : tok_rows + 1]
        + conv_taps[2] * padded[2 : tok_rows + 2]
    )
    conv_y = (gate_b.astype(jnp.float32) * convolved).astype(jnp.bfloat16)
    query_segment = token_index // SEG
    last_segment = (offset + tok_rows - 1) // SEG

    def key_block(running, latent_block, rot_block, first_key):
        peak_old, denom_old, accum_old = running
        block_rows = latent_block.shape[0]
        scores = (
            jnp.einsum(
                "thk,jk->thj", query_latent, latent_block, preferred_element_type=jnp.float32
            )
            + jnp.einsum("thr,jr->thj", query_rot, rot_block, preferred_element_type=jnp.float32)
        ) * attn_scale
        key_segment = (first_key + jnp.arange(block_rows, dtype=jnp.int32)) // SEG
        allowed = key_segment[None, None, :] <= query_segment[:, None, None]
        peak_new = jnp.maximum(peak_old, jnp.max(jnp.where(allowed, scores, -1e30), axis=-1))
        weights = jnp.where(allowed, jnp.exp(scores - peak_new[..., None]), 0.0)
        rescale = jnp.exp(peak_old - peak_new)
        denom_new = denom_old * rescale + jnp.sum(weights, axis=-1)
        accum_new = accum_old * rescale[..., None] + jnp.einsum(
            "thj,jk->thk",
            weights.astype(jnp.bfloat16),
            latent_block,
            preferred_element_type=jnp.float32,
        )
        return (peak_new, denom_new, accum_new)

    starting = (
        jnp.full((tok_rows, local_heads), -1e30, jnp.float32),
        jnp.zeros((tok_rows, local_heads), jnp.float32),
        jnp.zeros((tok_rows, local_heads, KVL), jnp.float32),
    )
    latent_piece = lax.all_gather(latent, "sp", axis=0, tiled=True)
    rot_piece = lax.all_gather(key_rot, "sp", axis=0, tiled=True)
    piece_rows = latent_piece.shape[0]
    splits = max(1, piece_rows // 512)
    while piece_rows % splits:
        splits = splits - 1
    block_rows = piece_rows // splits

    def visit(state, block_index):
        block_begin = block_index * block_rows
        latent_block = lax.dynamic_slice_in_dim(latent_piece, block_begin, block_rows, 0)
        rot_block = lax.dynamic_slice_in_dim(rot_piece, block_begin, block_rows, 0)
        updated = lax.cond(
            block_begin // SEG <= last_segment,
            lambda inner: key_block(inner, latent_block, rot_block, block_begin),
            lambda inner: inner,
            state,
        )
        return (updated, None)

    peak, denom, accum = lax.scan(visit, starting, jnp.arange(splits, dtype=jnp.int32))[0]
    attended = (accum / denom[..., None]).astype(jnp.bfloat16)
    head_out = jnp.einsum(
        "thk,khv->thv",
        attended,
        value_up_weight.reshape(KVL, local_heads, VD),
        preferred_element_type=jnp.float32,
    )
    normed_heads = rms_scale(head_out, head_gain.reshape(local_heads, VD))
    attn_y = normed_heads.astype(jnp.bfloat16).reshape(tok_rows, local_heads * VD)
    share_rows = tok_rows // count_tp
    conv_all, attn_all = (
        lax.all_gather(conv_y, "fs", axis=0, tiled=True),
        lax.all_gather(attn_y, "fs", axis=0, tiled=True),
    )
    conv_sorted = (
        conv_all.reshape(count_fs, count_tp, share_rows, -1)
        .transpose(1, 0, 2, 3)
        .reshape(count_fs * tok_rows, -1)
    )
    attn_sorted = (
        attn_all.reshape(count_fs, count_tp, share_rows, -1)
        .transpose(1, 0, 2, 3)
        .reshape(count_fs * tok_rows, -1)
    )
    conv_cols_sp, attn_cols_sp = (
        lax.all_gather(conv_out_weight, "sp", axis=1, tiled=True),
        lax.all_gather(attn_out_weight, "sp", axis=1, tiled=True),
    )
    col_sums = lax.psum_scatter(
        (
            jnp.dot(conv_sorted, conv_cols_sp, preferred_element_type=jnp.float32)
            + jnp.dot(attn_sorted, attn_cols_sp, preferred_element_type=jnp.float32)
        ).astype(jnp.bfloat16),
        "tp",
        scatter_dimension=0,
        tiled=True,
    )
    col_piece = conv_cols_sp.shape[1] // count_sp
    outgoing = col_sums.reshape(count_fs, share_rows, count_sp * col_piece)
    arrived = lax.all_to_all(outgoing, "fs", split_axis=0, concat_axis=2, tiled=True)
    result = (
        arrived.reshape(share_rows, count_fs, count_sp, col_piece)
        .transpose(0, 2, 1, 3)
        .reshape(share_rows, count_fs * count_sp * col_piece)
    )
    return result[None]


def turned(block, axis, distance):
    count = lax.axis_size(axis)
    return lax.ppermute(block, axis, [(i, (i + distance) % count) for i in range(count)])


def swapped(block, axis, mask):
    return lax.ppermute(block, axis, [(i, i ^ mask) for i in range(lax.axis_size(axis))])


def after(values, *others):
    return lax.optimization_barrier((values,) + others)[0]


def exchange(blocks, axis):
    return [blocks[0]] + [turned(blocks[d], axis, d) for d in range(1, len(blocks))]


def spread(block):
    by_one = swapped(block, "fs", 1)
    by_two = swapped(block, "fs", 2)
    half = block.shape[0] // 2
    upper = swapped(by_one[:half], "fs", 2)
    lower = swapped(by_two[half:], "fs", 1)
    return [[block], [by_one], [by_two], [upper, lower]]


def in_vmem(count):
    return [pl.BlockSpec(memory_space=pltpu.VMEM) for _ in range(count)]


def local_kernel(body, outs, scalars, *arrays):
    return pl.pallas_call(
        body,
        in_specs=[pl.BlockSpec(memory_space=pltpu.SMEM)] + in_vmem(len(arrays)),
        out_specs=in_vmem(len(outs)),
        out_shape=[jax.ShapeDtypeStruct(shape, jnp.bfloat16) for shape in outs],
    )(scalars, *arrays)


def pack_columns(index, count, groups):
    flat = [w for group in groups for w in group]
    rows = flat[0].shape[0]
    widths = [[w.shape[1] // count for w in group] for group in groups]
    outs = [(rows, sum(widths[g])) for g in range(len(groups)) for _ in range(count)]
    targets = (index + jnp.arange(count, dtype=jnp.int32)) % count

    def body(target_ref, *refs):
        ins, out_refs = refs[: len(flat)], refs[len(flat) :]
        taken = 0
        for g, group in enumerate(groups):
            for d in range(count):
                out = out_refs[g * count + d]
                begin = 0
                for i, width in enumerate(widths[g]):
                    source = pl.multiple_of(target_ref[d] * width, width)
                    out[:, begin : begin + width] = ins[taken + i][:, pl.ds(source, width)]
                    begin += width
            taken += len(group)

    made = local_kernel(body, outs, targets, *flat)
    return [made[g * count : (g + 1) * count] for g in range(len(groups))]


def norm_columns(halves, others, gain, key_rope, tp_index, sp_index, order):
    count = len(halves)
    rows, half = halves[0].shape
    pieces = order.shape[0]
    width = 2 * half // pieces
    per_half = pieces // 2
    scalars = jnp.concatenate(
        [
            order,
            (sp_index - jnp.arange(count, dtype=jnp.int32)) % count,
            tp_index[None].astype(jnp.int32),
        ]
    )

    def body(scalar_ref, gain_ref, rope_ref, *refs):
        ins, (out, rope_out) = refs[: 2 * count], refs[2 * count :]
        side = scalar_ref[pieces + count]
        for d in range(count):
            mine, other = ins[d], ins[count + d]
            row = pl.multiple_of(scalar_ref[pieces + d] * rows, rows)
            square = jnp.zeros((rows, 1), jnp.float32)
            for ref in (mine, other):
                values = ref[...].astype(jnp.float32)
                square += jnp.sum(values * values, axis=1, keepdims=True)
            scale = lax.rsqrt(square / (2 * half) + norm_epsilon)
            for j in range(pieces):
                piece = scalar_ref[j]
                column = pl.multiple_of((piece % per_half) * width, width)
                local = mine[:, pl.ds(column, width)].astype(jnp.float32)
                far = other[:, pl.ds(column, width)].astype(jnp.float32)
                values = jnp.where(piece // per_half == side, local, far)
                factor = gain_ref[:, pl.ds(pl.multiple_of(piece * width, width), width)]
                out[pl.ds(row, rows), j * width : (j + 1) * width] = (
                    values * scale * factor
                ).astype(jnp.bfloat16)
        for j in range(pieces):
            begin = pl.multiple_of(scalar_ref[j] * width, width)
            rope_out[j * width : (j + 1) * width, :] = rope_ref[pl.ds(begin, width), :]

    outs = [(count * rows, 2 * half), key_rope.shape]
    return local_kernel(body, outs, scalars, gain[None, :], key_rope, *halves, *others)


def place_columns(blocks, order):
    rows, width = blocks[0].shape

    def body(order_ref, *refs):
        out = refs[-1]
        for i in range(len(blocks)):
            out[:, pl.ds(pl.multiple_of(order_ref[i] * width, width), width)] = refs[i][...]

    return local_kernel(body, [(rows, width * len(blocks))], order, *blocks)[0]


def head_parallel(
    tokens,
    mix_gain,
    conv_b_weight,
    conv_c_weight,
    conv_v_weight,
    conv_taps,
    query_weight,
    query_rope_weight,
    latent_weight,
    key_rope_weight,
    latent_gain,
    key_up_weight,
    value_up_weight,
    head_gain,
    conv_out_weight,
    attn_out_weight,
):
    count_sp = lax.axis_size("sp")
    count_fs = lax.axis_size("fs")
    count_tp = lax.axis_size("tp")
    sp_index = lax.axis_index("sp")
    fs_index = lax.axis_index("fs")
    tp_index = lax.axis_index("tp")
    bf16 = jnp.bfloat16
    f32 = jnp.float32
    tok_rows = tokens.shape[1]
    length = tok_rows * count_sp
    row_piece = query_weight.shape[0]
    heads = query_weight.shape[1] // NOPE // count_sp
    chans = conv_b_weight.shape[1] // count_sp
    lat_cols = latent_weight.shape[1] // count_sp
    sources = (sp_index - jnp.arange(count_sp, dtype=jnp.int32)) % count_sp
    faces = fs_index ^ jnp.arange(count_fs, dtype=jnp.int32)
    order = (sources[None, :] * count_fs + faces[:, None]).reshape(-1)

    pack_attn, pack_conv = pack_columns(
        sp_index,
        count_sp,
        (
            (query_weight, query_rope_weight, latent_weight),
            (conv_b_weight, conv_c_weight, conv_v_weight),
        ),
    )
    arrived_attn = exchange(pack_attn, "sp")
    parts_attn = spread(jnp.concatenate(arrived_attn, axis=0))

    own = after(tokens[0], *arrived_attn)
    halves = [own] + [turned(own, "sp", d) for d in range(1, count_sp)]
    others = [swapped(half, "tp", 1) for half in halves]
    normed, key_rope = norm_columns(
        halves, others, mix_gain, key_rope_weight, tp_index, sp_index, order
    )

    pack_conv = [after(block, *halves) for block in pack_conv]
    arrived_conv = exchange(pack_conv, "sp")
    joined_conv = jnp.concatenate(arrived_conv, axis=0)
    parts_conv = spread(after(joined_conv, *[p for part in parts_attn for p in part]))

    def project(parts):
        total = 0.0
        begin = 0
        for part in parts:
            for piece in part:
                columns = normed[:, begin : begin + piece.shape[0]]
                total = total + jnp.dot(columns, piece, preferred_element_type=f32)
                begin += piece.shape[0]
        return total

    attn_in = project(parts_attn)
    edge_rot = heads * NOPE
    edge_lat = edge_rot + heads * ROPE
    lat_rows = length // count_tp
    lat_own = lax.dynamic_slice_in_dim(
        attn_in[:, edge_lat:].astype(bf16), tp_index * lat_rows, lat_rows, 0
    )
    lat_blocks = [lat_own] + [turned(lat_own, "sp", d) for d in range(1, count_sp)]
    lat_mine = jnp.concatenate(lat_blocks, axis=1)
    lat_other = swapped(lat_mine, "tp", 1)
    latent_raw = jnp.where(
        tp_index == 0,
        jnp.concatenate([lat_mine, lat_other], axis=0),
        jnp.concatenate([lat_other, lat_mine], axis=0),
    )

    def turned_rows(weight, width, begin):
        return jnp.concatenate(
            [
                lax.dynamic_slice(weight, (sources[d] * lat_cols, begin), (lat_cols, width))
                for d in range(count_sp)
            ],
            axis=0,
        )

    lat_gain = turned_rows(latent_gain[:, None], 1, 0)[:, 0]
    latent = rms_scale(latent_raw.astype(f32), lat_gain).astype(bf16)

    position = jnp.arange(length, dtype=jnp.int32)
    cosine, sine = rope_tables(position.astype(f32))
    key_rot = rotate(
        jnp.dot(normed, key_rope, preferred_element_type=f32), cosine, sine
    ).astype(bf16)

    key_up = turned_rows(key_up_weight, heads * NOPE, sp_index * heads * NOPE)
    value_up = turned_rows(value_up_weight, heads * VD, sp_index * heads * VD)
    gain = lax.dynamic_slice_in_dim(head_gain, sp_index * heads * VD, heads * VD, 0)
    taps = lax.dynamic_slice_in_dim(conv_taps, sp_index * chans, chans, 1)

    out_rows = []
    for d in range(count_sp):
        target = (sp_index + d) % count_sp
        out_rows.append(
            jnp.concatenate(
                [
                    lax.dynamic_slice_in_dim(conv_out_weight, target * chans, chans, 0),
                    lax.dynamic_slice_in_dim(
                        attn_out_weight, target * heads * VD, heads * VD, 0
                    ),
                ],
                axis=0,
            )
        )
    out_rows = [after(block, *arrived_conv, *lat_blocks) for block in out_rows]
    arrived_out = jnp.concatenate(exchange(out_rows, "sp"), axis=0)
    parts_out = spread(after(arrived_out, *[p for part in parts_conv for p in part]))
    out_height = chans + heads * VD
    out_blocks = [
        piece[i : i + out_height]
        for part in parts_out
        for piece in part
        for i in range(0, piece.shape[0], out_height)
    ]
    out_weight = place_columns(out_blocks, order)

    conv_in = project(parts_conv).astype(bf16).astype(f32)
    gate_b = conv_in[:, :chans]
    product = (conv_in[:, chans : 2 * chans] * conv_in[:, 2 * chans :]).astype(bf16)
    padded = jnp.concatenate([jnp.zeros((2, chans), bf16), product], axis=0).astype(f32)
    convolved = (
        taps[0] * padded[0:length] + taps[1] * padded[1 : length + 1] + taps[2] * padded[2:]
    )
    conv_y = (gate_b * convolved).astype(bf16)

    attn_scale = (NOPE + ROPE) ** (-0.5)
    segment = position // SEG
    allowed = segment[None, :] <= segment[:, None]
    mixers = [conv_y]
    for h in range(heads):
        query_nope = attn_in[:, h * NOPE : (h + 1) * NOPE].astype(bf16)
        query_rot = rotate(
            attn_in[:, edge_rot + h * ROPE : edge_rot + (h + 1) * ROPE], cosine, sine
        ).astype(bf16)
        query_latent = lax.dot_general(
            query_nope,
            key_up[:, h * NOPE : (h + 1) * NOPE],
            (((1,), (1,)), ((), ())),
            preferred_element_type=f32,
        ).astype(bf16)
        scores = (
            lax.dot_general(
                query_latent, latent, (((1,), (1,)), ((), ())), preferred_element_type=f32
            )
            + lax.dot_general(
                query_rot, key_rot, (((1,), (1,)), ((), ())), preferred_element_type=f32
            )
        ) * attn_scale
        scores = jnp.where(allowed, scores, -1e30)
        top = jnp.max(scores, axis=-1, keepdims=True)
        weights = jnp.where(allowed, jnp.exp(scores - top), 0.0)
        total = jnp.sum(weights, axis=-1, keepdims=True)
        accum = jnp.dot(weights.astype(bf16), latent, preferred_element_type=f32)
        attended = (accum / total).astype(bf16)
        head_out = jnp.dot(
            attended, value_up[:, h * VD : (h + 1) * VD], preferred_element_type=f32
        )
        mixers.append(rms_scale(head_out, gain[h * VD : (h + 1) * VD]).astype(bf16))
    mixers = jnp.concatenate(mixers, axis=1)

    share = tok_rows // count_tp
    final = None
    for distance in [*range(count_sp - 1, 0, -1), 0]:
        target = (sp_index + distance) % count_sp

        def partial(side):
            rows = lax.dynamic_slice_in_dim(
                mixers, target * tok_rows + side * share, share, 0
            )
            return jnp.dot(rows, out_weight, preferred_element_type=f32).astype(bf16)

        both = partial(tp_index).astype(f32) + swapped(partial(1 - tp_index), "tp", 1).astype(f32)
        if distance:
            both = turned(both.astype(bf16), "sp", distance).astype(f32)
        final = both if final is None else final + both
    return final.astype(bf16)[None]


def solution(mesh):
    sizes = dict(mesh.shape)
    divided = sizes["sp"] * sizes["tp"]
    fits = sizes["tp"] == 2 and sizes["fs"] == 4

    def shards(*args):
        heads = args[6].shape[1] // NOPE
        chans = args[2].shape[1]
        even = heads % sizes["sp"] == 0 and chans % sizes["sp"] == 0 and KVL % divided == 0
        even = even and sizes["sp"] % 2 == 0 and chans // sizes["sp"] % 128 == 0
        if fits and even:
            return head_parallel(*args)
        return token_parallel(*args)

    return jax.shard_map(
        shards,
        mesh=mesh,
        in_specs=(
            P("fs", "sp", "tp"),
            P(),
            P(("sp", "fs"), "tp"),
            P(("sp", "fs"), "tp"),
            P(("sp", "fs"), "tp"),
            P(None, "tp"),
            P(("sp", "fs"), "tp"),
            P(("sp", "fs"), "tp"),
            P(("sp", "fs"), None),
            P(),
            P(),
            P(None, "tp"),
            P(None, "tp"),
            P("tp"),
            P("tp", ("sp", "fs")),
            P("tp", ("sp", "fs")),
        ),
        out_specs=P("fs", ("sp", "tp"), None),
        check_vma=False,
    )
```

```python
import jax
import jax.numpy as jnp
from jax import lax
from jax.experimental import pallas as pl
from jax.experimental.pallas import tpu as pltpu
from jax.sharding import PartitionSpec as P

NOPE = 128
ROPE = 64
VD = 128
KVL = 512
SEG = 64


norm_epsilon = 1e-06
rope_theta = 10000.0


def passed_along(block, axis, distance):
    devices = range(lax.axis_size(axis))
    route = [(i - distance, i) for i in devices if i - distance in devices]
    return lax.ppermute(block, axis, route)


def rms_scale(values, gain):
    return (
        values * lax.rsqrt(jnp.mean(values * values, axis=-1, keepdims=True) + norm_epsilon) * gain
    )


def rope_tables(positions):
    half_width = ROPE // 2
    frequency = rope_theta ** (-jnp.arange(half_width, dtype=jnp.float32) * 2.0 / ROPE)
    angles = positions[:, None] * frequency[None, :]
    return (jnp.cos(angles), jnp.sin(angles))


def rotate(values, cosine, sine):
    half_width = ROPE // 2
    first = values[..., :half_width]
    second = values[..., half_width:]
    return jnp.concatenate(
        [first * cosine - second * sine, second * cosine + first * sine], axis=-1
    )


def token_parallel(
    tokens,
    mix_gain,
    conv_b_weight,
    conv_c_weight,
    conv_v_weight,
    conv_taps,
    query_weight,
    query_rope_weight,
    latent_weight,
    key_rope_weight,
    latent_gain,
    key_up_weight,
    value_up_weight,
    head_gain,
    conv_out_weight,
    attn_out_weight,
):
    full_rows = lax.all_gather(tokens[0], "tp", axis=1, tiled=True)
    tok_rows = full_rows.shape[0]
    normed = rms_scale(full_rows.astype(jnp.float32), mix_gain).astype(jnp.bfloat16)
    offset = lax.axis_index("sp") * tok_rows
    token_index = offset + jnp.arange(tok_rows, dtype=jnp.int32)
    cosine, sine = rope_tables(token_index.astype(jnp.float32))
    local_heads = query_weight.shape[1] // NOPE
    count_sp = lax.axis_size("sp")
    count_fs = lax.axis_size("fs")
    count_tp = lax.axis_size("tp")
    fs_index = lax.axis_index("fs")
    row_piece = normed.shape[1] // (count_sp * count_fs)
    all_normed = lax.all_gather(normed, "fs", axis=0, tiled=True)
    picked = lax.dynamic_index_in_dim(
        all_normed.reshape(-1, count_sp, count_fs, row_piece), fs_index, 2, keepdims=False
    ).reshape(-1, count_sp * row_piece)
    gathered = (
        lax.all_gather(conv_b_weight, "sp", axis=0, tiled=True),
        lax.all_gather(conv_c_weight, "sp", axis=0, tiled=True),
        lax.all_gather(conv_v_weight, "sp", axis=0, tiled=True),
        lax.all_gather(query_weight, "sp", axis=0, tiled=True),
        lax.all_gather(query_rope_weight, "sp", axis=0, tiled=True),
        lax.all_gather(latent_weight, "sp", axis=0, tiled=True),
    )

    def project_in():
        return jnp.concatenate(
            [jnp.dot(picked, member, preferred_element_type=jnp.float32) for member in gathered],
            axis=1,
        )

    joined = lax.psum_scatter(
        project_in().astype(jnp.bfloat16), "fs", scatter_dimension=0, tiled=True
    ).astype(jnp.float32)
    bounds = []
    running_total = 0
    for member in gathered[:-1]:
        running_total = running_total + member.shape[1]
        bounds.append(running_total)
    sums = tuple(jnp.split(joined, bounds, axis=1))
    latent_raw = sums[5].astype(jnp.bfloat16)
    gate_b = sums[0].astype(jnp.bfloat16)
    gate_c = sums[1].astype(jnp.bfloat16)
    values_v = sums[2].astype(jnp.bfloat16)
    query_nope = sums[3].astype(jnp.bfloat16).reshape(tok_rows, local_heads, NOPE)
    query_rot = rotate(
        sums[4].reshape(tok_rows, local_heads, ROPE), cosine[:, None, :], sine[:, None, :]
    ).astype(jnp.bfloat16)
    latent = rms_scale(latent_raw.astype(jnp.float32), latent_gain).astype(jnp.bfloat16)
    key_rot = rotate(
        jnp.dot(normed, key_rope_weight, preferred_element_type=jnp.float32), cosine, sine
    ).astype(jnp.bfloat16)
    query_latent = jnp.einsum(
        "thn,khn->thk",
        query_nope,
        key_up_weight.reshape(KVL, local_heads, NOPE),
        preferred_element_type=jnp.float32,
    ).astype(jnp.bfloat16)
    attn_scale = (NOPE + ROPE) ** (-0.5)
    product = (gate_c.astype(jnp.float32) * values_v.astype(jnp.float32)).astype(jnp.bfloat16)
    previous = passed_along(product[tok_rows - 2 :], "sp", 1)
    padded = jnp.concatenate([previous, product], axis=0).astype(jnp.float32)
    convolved = (
        conv_taps[0] * padded[0:tok_rows]
        + conv_taps[1] * padded[1 : tok_rows + 1]
        + conv_taps[2] * padded[2 : tok_rows + 2]
    )
    conv_y = (gate_b.astype(jnp.float32) * convolved).astype(jnp.bfloat16)
    query_segment = token_index // SEG
    last_segment = (offset + tok_rows - 1) // SEG

    def key_block(running, latent_block, rot_block, first_key):
        peak_old, denom_old, accum_old = running
        block_rows = latent_block.shape[0]
        scores = (
            jnp.einsum(
                "thk,jk->thj", query_latent, latent_block, preferred_element_type=jnp.float32
            )
            + jnp.einsum("thr,jr->thj", query_rot, rot_block, preferred_element_type=jnp.float32)
        ) * attn_scale
        key_segment = (first_key + jnp.arange(block_rows, dtype=jnp.int32)) // SEG
        allowed = key_segment[None, None, :] <= query_segment[:, None, None]
        peak_new = jnp.maximum(peak_old, jnp.max(jnp.where(allowed, scores, -1e30), axis=-1))
        weights = jnp.where(allowed, jnp.exp(scores - peak_new[..., None]), 0.0)
        rescale = jnp.exp(peak_old - peak_new)
        denom_new = denom_old * rescale + jnp.sum(weights, axis=-1)
        accum_new = accum_old * rescale[..., None] + jnp.einsum(
            "thj,jk->thk",
            weights.astype(jnp.bfloat16),
            latent_block,
            preferred_element_type=jnp.float32,
        )
        return (peak_new, denom_new, accum_new)

    starting = (
        jnp.full((tok_rows, local_heads), -1e30, jnp.float32),
        jnp.zeros((tok_rows, local_heads), jnp.float32),
        jnp.zeros((tok_rows, local_heads, KVL), jnp.float32),
    )
    latent_piece = lax.all_gather(latent, "sp", axis=0, tiled=True)
    rot_piece = lax.all_gather(key_rot, "sp", axis=0, tiled=True)
    piece_rows = latent_piece.shape[0]
    splits = max(1, piece_rows // 512)
    while piece_rows % splits:
        splits = splits - 1
    block_rows = piece_rows // splits

    def visit(state, block_index):
        block_begin = block_index * block_rows
        latent_block = lax.dynamic_slice_in_dim(latent_piece, block_begin, block_rows, 0)
        rot_block = lax.dynamic_slice_in_dim(rot_piece, block_begin, block_rows, 0)
        updated = lax.cond(
            block_begin // SEG <= last_segment,
            lambda inner: key_block(inner, latent_block, rot_block, block_begin),
            lambda inner: inner,
            state,
        )
        return (updated, None)

    peak, denom, accum = lax.scan(visit, starting, jnp.arange(splits, dtype=jnp.int32))[0]
    attended = (accum / denom[..., None]).astype(jnp.bfloat16)
    head_out = jnp.einsum(
        "thk,khv->thv",
        attended,
        value_up_weight.reshape(KVL, local_heads, VD),
        preferred_element_type=jnp.float32,
    )
    normed_heads = rms_scale(head_out, head_gain.reshape(local_heads, VD))
    attn_y = normed_heads.astype(jnp.bfloat16).reshape(tok_rows, local_heads * VD)
    share_rows = tok_rows // count_tp
    conv_all, attn_all = (
        lax.all_gather(conv_y, "fs", axis=0, tiled=True),
        lax.all_gather(attn_y, "fs", axis=0, tiled=True),
    )
    conv_sorted = (
        conv_all.reshape(count_fs, count_tp, share_rows, -1)
        .transpose(1, 0, 2, 3)
        .reshape(count_fs * tok_rows, -1)
    )
    attn_sorted = (
        attn_all.reshape(count_fs, count_tp, share_rows, -1)
        .transpose(1, 0, 2, 3)
        .reshape(count_fs * tok_rows, -1)
    )
    conv_cols_sp, attn_cols_sp = (
        lax.all_gather(conv_out_weight, "sp", axis=1, tiled=True),
        lax.all_gather(attn_out_weight, "sp", axis=1, tiled=True),
    )
    col_sums = lax.psum_scatter(
        (
            jnp.dot(conv_sorted, conv_cols_sp, preferred_element_type=jnp.float32)
            + jnp.dot(attn_sorted, attn_cols_sp, preferred_element_type=jnp.float32)
        ).astype(jnp.bfloat16),
        "tp",
        scatter_dimension=0,
        tiled=True,
    )
    col_piece = conv_cols_sp.shape[1] // count_sp
    outgoing = col_sums.reshape(count_fs, share_rows, count_sp * col_piece)
    arrived = lax.all_to_all(outgoing, "fs", split_axis=0, concat_axis=2, tiled=True)
    result = (
        arrived.reshape(share_rows, count_fs, count_sp, col_piece)
        .transpose(0, 2, 1, 3)
        .reshape(share_rows, count_fs * count_sp * col_piece)
    )
    return result[None]


def turned(block, axis, distance):
    count = lax.axis_size(axis)
    return lax.ppermute(block, axis, [(i, (i + distance) % count) for i in range(count)])


def swapped(block, axis, mask):
    return lax.ppermute(block, axis, [(i, i ^ mask) for i in range(lax.axis_size(axis))])


def after(values, *others):
    return lax.optimization_barrier((values,) + others)[0]


def exchange(blocks, axis):
    return [blocks[0]] + [turned(blocks[d], axis, d) for d in range(1, len(blocks))]


def spread(block):
    by_one = swapped(block, "fs", 1)
    by_two = swapped(block, "fs", 2)
    half = block.shape[0] // 2
    upper = swapped(by_one[:half], "fs", 2)
    lower = swapped(by_two[half:], "fs", 1)
    return [[block], [by_one], [by_two], [upper, lower]]


def in_vmem(count):
    return [pl.BlockSpec(memory_space=pltpu.VMEM) for _ in range(count)]


def local_kernel(body, outs, scalars, *arrays):
    return pl.pallas_call(
        body,
        in_specs=[pl.BlockSpec(memory_space=pltpu.SMEM)] + in_vmem(len(arrays)),
        out_specs=in_vmem(len(outs)),
        out_shape=[jax.ShapeDtypeStruct(shape, jnp.bfloat16) for shape in outs],
    )(scalars, *arrays)


def pack_columns(index, count, groups, stacked):
    flat = [w for group in groups for w in group]
    rows = flat[0].shape[0]
    widths = [[w.shape[1] // count for w in group] for group in groups]
    stacks = [(w.shape[0] // count // rows, w.shape[1]) for w in stacked]
    tail = sum(pieces * width for pieces, width in stacks)
    full = [sum(group) for group in widths]
    full[-1] += tail
    outs = [(rows, full[g]) for g in range(len(groups)) for _ in range(count)]
    inputs = len(flat) + len(stacked)
    targets = (index + jnp.arange(count, dtype=jnp.int32)) % count

    def body(target_ref, *refs):
        ins, out_refs = refs[:inputs], refs[inputs:]
        taken = 0
        for g, group in enumerate(groups):
            for d in range(count):
                out = out_refs[g * count + d]
                begin = 0
                for i, width in enumerate(widths[g]):
                    source = pl.multiple_of(target_ref[d] * width, width)
                    out[:, begin : begin + width] = ins[taken + i][:, pl.ds(source, width)]
                    begin += width
            taken += len(group)
        for d in range(count):
            out = out_refs[(len(groups) - 1) * count + d]
            begin = sum(widths[-1])
            for i, (pieces, width) in enumerate(stacks):
                for j in range(pieces):
                    source = pl.multiple_of((target_ref[d] * pieces + j) * rows, rows)
                    out[:, begin : begin + width] = ins[len(flat) + i][pl.ds(source, rows), :]
                    begin += width

    made = local_kernel(body, outs, targets, *flat, *stacked)
    return [made[g * count : (g + 1) * count] for g in range(len(groups))]


def norm_columns(halves, others, gain, key_rope, tp_index, sp_index, order):
    count = len(halves)
    rows, half = halves[0].shape
    pieces = order.shape[0]
    width = 2 * half // pieces
    per_half = pieces // 2
    scalars = jnp.concatenate(
        [
            order,
            (sp_index - jnp.arange(count, dtype=jnp.int32)) % count,
            tp_index[None].astype(jnp.int32),
        ]
    )

    def body(scalar_ref, gain_ref, rope_ref, *refs):
        ins, (out, rope_out) = refs[: 2 * count], refs[2 * count :]
        side = scalar_ref[pieces + count]
        for d in range(count):
            mine, other = ins[d], ins[count + d]
            row = pl.multiple_of(scalar_ref[pieces + d] * rows, rows)
            square = jnp.zeros((rows, 1), jnp.float32)
            for ref in (mine, other):
                values = ref[...].astype(jnp.float32)
                square += jnp.sum(values * values, axis=1, keepdims=True)
            scale = lax.rsqrt(square / (2 * half) + norm_epsilon)
            for j in range(pieces):
                piece = scalar_ref[j]
                column = pl.multiple_of((piece % per_half) * width, width)
                local = mine[:, pl.ds(column, width)].astype(jnp.float32)
                far = other[:, pl.ds(column, width)].astype(jnp.float32)
                values = jnp.where(piece // per_half == side, local, far)
                factor = gain_ref[:, pl.ds(pl.multiple_of(piece * width, width), width)]
                out[pl.ds(row, rows), j * width : (j + 1) * width] = (
                    values * scale * factor
                ).astype(jnp.bfloat16)
        for j in range(pieces):
            begin = pl.multiple_of(scalar_ref[j] * width, width)
            rope_out[j * width : (j + 1) * width, :] = rope_ref[pl.ds(begin, width), :]

    outs = [(count * rows, 2 * half), key_rope.shape]
    return local_kernel(body, outs, scalars, gain[None, :], key_rope, *halves, *others)


def place_columns(parts, order, begin, rows, width):
    pieces = (parts[0].shape[1] - begin) // width
    places = order.shape[0]

    def body(order_ref, *refs):
        out = refs[-1]
        place = 0
        for ref in refs[:-1]:
            for top in range(0, ref.shape[0], rows):
                column = pl.multiple_of(order_ref[place] * width, width)
                for j in range(pieces):
                    left = begin + j * width
                    out[j * rows : (j + 1) * rows, pl.ds(column, width)] = ref[
                        top : top + rows, left : left + width
                    ]
                place += 1

    return local_kernel(body, [(pieces * rows, places * width)], order, *parts)[0]


def mix_block(target, tp_index, rows, query, query_rot, latent, key_rot, key_up, value_up, gain, conv_y, out_weight):
    heads = query.shape[1] // NOPE
    length = latent.shape[0]
    chans = conv_y.shape[1]
    columns = out_weight.shape[1]
    attn_scale = (NOPE + ROPE) ** (-0.5)
    transposed = (((1,), (1,)), ((), ()))

    def dot(left, right, dims=(((1,), (0,)), ((), ()))):
        return lax.dot_general(left, right, dims, preferred_element_type=jnp.float32)

    def body(s_ref, q_ref, qr_ref, lat_ref, kr_ref, ku_ref, vu_ref, g_ref, c_ref, w_ref, keep_ref, give_ref):
        row = pl.multiple_of(s_ref[0] * rows, rows)
        latents = lat_ref[...]
        keys_rot = kr_ref[...]
        own = (row + lax.broadcasted_iota(jnp.int32, (rows, length), 0)) // SEG
        theirs = lax.broadcasted_iota(jnp.int32, (rows, length), 1) // SEG
        allowed = theirs <= own
        mixed = dot(c_ref[pl.ds(row, rows), :], w_ref[:chans, :])
        for h in range(heads):
            low = dot(
                q_ref[pl.ds(row, rows), h * NOPE : (h + 1) * NOPE],
                ku_ref[:, h * NOPE : (h + 1) * NOPE],
                transposed,
            ).astype(jnp.bfloat16)
            rot = qr_ref[pl.ds(row, rows), h * ROPE : (h + 1) * ROPE]
            scores = (dot(low, latents, transposed) + dot(rot, keys_rot, transposed)) * attn_scale
            scores = jnp.where(allowed, scores, -1e30)
            top = jnp.max(scores, axis=-1, keepdims=True)
            weights = jnp.where(allowed, jnp.exp(scores - top), 0.0)
            total = jnp.sum(weights, axis=-1, keepdims=True)
            attended = (dot(weights.astype(jnp.bfloat16), latents) / total).astype(jnp.bfloat16)
            head_out = dot(attended, vu_ref[:, h * VD : (h + 1) * VD])
            attn_y = rms_scale(head_out, g_ref[:, h * VD : (h + 1) * VD]).astype(jnp.bfloat16)
            begin = chans + h * VD
            mixed += dot(attn_y, w_ref[begin : begin + VD, :])
        low_half = mixed[: rows // 2].astype(jnp.bfloat16)
        high_half = mixed[rows // 2 :].astype(jnp.bfloat16)
        first = s_ref[1] == 0
        keep_ref[...] = jnp.where(first, low_half, high_half)
        give_ref[...] = jnp.where(first, high_half, low_half)

    flops = 2 * rows * (
        heads * (length * (2 * KVL + ROPE) + KVL * (NOPE + VD)) + out_weight.shape[0] * columns
    )
    operands = (query, query_rot, latent, key_rot, key_up, value_up, gain[None, :], conv_y, out_weight)
    return pl.pallas_call(
        body,
        in_specs=[pl.BlockSpec(memory_space=pltpu.SMEM)] + in_vmem(len(operands)),
        out_specs=in_vmem(2),
        out_shape=[jax.ShapeDtypeStruct((rows // 2, columns), jnp.bfloat16)] * 2,
        cost_estimate=pl.CostEstimate(
            flops=flops, bytes_accessed=8 * rows * columns, transcendentals=heads * rows * length
        ),
    )(jnp.stack([target, tp_index]).astype(jnp.int32), *operands)


def head_parallel(
    tokens,
    mix_gain,
    conv_b_weight,
    conv_c_weight,
    conv_v_weight,
    conv_taps,
    query_weight,
    query_rope_weight,
    latent_weight,
    key_rope_weight,
    latent_gain,
    key_up_weight,
    value_up_weight,
    head_gain,
    conv_out_weight,
    attn_out_weight,
):
    count_sp = lax.axis_size("sp")
    count_fs = lax.axis_size("fs")
    count_tp = lax.axis_size("tp")
    sp_index = lax.axis_index("sp")
    fs_index = lax.axis_index("fs")
    tp_index = lax.axis_index("tp")
    bf16 = jnp.bfloat16
    f32 = jnp.float32
    tok_rows = tokens.shape[1]
    length = tok_rows * count_sp
    row_piece = query_weight.shape[0]
    heads = query_weight.shape[1] // NOPE // count_sp
    chans = conv_b_weight.shape[1] // count_sp
    lat_cols = latent_weight.shape[1] // count_sp
    sources = (sp_index - jnp.arange(count_sp, dtype=jnp.int32)) % count_sp
    faces = fs_index ^ jnp.arange(count_fs, dtype=jnp.int32)
    order = (sources[None, :] * count_fs + faces[:, None]).reshape(-1)

    pack_attn, pack_conv = pack_columns(
        sp_index,
        count_sp,
        (
            (query_weight, query_rope_weight, latent_weight),
            (conv_b_weight, conv_c_weight, conv_v_weight),
        ),
        (conv_out_weight, attn_out_weight),
    )
    arrived_attn = exchange(pack_attn, "sp")
    parts_attn = spread(jnp.concatenate(arrived_attn, axis=0))

    pack_conv = [after(block, *arrived_attn) for block in pack_conv]
    arrived_conv = exchange(pack_conv, "sp")
    joined_conv = jnp.concatenate(arrived_conv, axis=0)
    pieces_attn = [p for part in parts_attn for p in part]
    parts_conv = spread(after(joined_conv, *pieces_attn))

    own = tokens[0]
    sent = after(own, *arrived_conv)
    halves = [own] + [turned(sent, "sp", d) for d in range(1, count_sp)]
    others = [swapped(half, "tp", 1) for half in halves]
    normed, key_rope = norm_columns(
        halves, others, mix_gain, key_rope_weight, tp_index, sp_index, order
    )

    def project(parts, width):
        total = 0.0
        begin = 0
        for part in parts:
            for piece in part:
                columns = normed[:, begin : begin + piece.shape[0]]
                total = total + jnp.dot(columns, piece[:, :width], preferred_element_type=f32)
                begin += piece.shape[0]
        return total

    attn_in = project(parts_attn, parts_attn[0][0].shape[1])
    edge_rot = heads * NOPE
    edge_lat = edge_rot + heads * ROPE
    lat_rows = length // count_tp
    lat_own = lax.dynamic_slice_in_dim(
        attn_in[:, edge_lat:].astype(bf16), tp_index * lat_rows, lat_rows, 0
    )
    lat_blocks = [lat_own] + [turned(lat_own, "sp", d) for d in range(1, count_sp)]
    lat_mine = jnp.concatenate(lat_blocks, axis=1)
    lat_other = swapped(lat_mine, "tp", 1)
    latent_raw = jnp.where(
        tp_index == 0,
        jnp.concatenate([lat_mine, lat_other], axis=0),
        jnp.concatenate([lat_other, lat_mine], axis=0),
    )

    def turned_rows(weight, width, begin):
        return jnp.concatenate(
            [
                lax.dynamic_slice(weight, (sources[d] * lat_cols, begin), (lat_cols, width))
                for d in range(count_sp)
            ],
            axis=0,
        )

    lat_gain = turned_rows(latent_gain[:, None], 1, 0)[:, 0]
    latent = rms_scale(latent_raw.astype(f32), lat_gain).astype(bf16)

    position = jnp.arange(length, dtype=jnp.int32)
    cosine, sine = rope_tables(position.astype(f32))
    key_rot = rotate(
        jnp.dot(normed, key_rope, preferred_element_type=f32), cosine, sine
    ).astype(bf16)

    key_up = turned_rows(key_up_weight, heads * NOPE, sp_index * heads * NOPE)
    value_up = turned_rows(value_up_weight, heads * VD, sp_index * heads * VD)
    gain = lax.dynamic_slice_in_dim(head_gain, sp_index * heads * VD, heads * VD, 0)
    taps = lax.dynamic_slice_in_dim(conv_taps, sp_index * chans, chans, 1)

    pieces_conv = [p for part in parts_conv for p in part]
    out_weight = place_columns(
        pieces_conv, order, 3 * chans, row_piece, conv_out_weight.shape[1]
    )

    conv_in = project(parts_conv, 3 * chans).astype(bf16).astype(f32)
    gate_b = conv_in[:, :chans]
    product = (conv_in[:, chans : 2 * chans] * conv_in[:, 2 * chans :]).astype(bf16)
    padded = jnp.concatenate([jnp.zeros((2, chans), bf16), product], axis=0).astype(f32)
    convolved = (
        taps[0] * padded[0:length] + taps[1] * padded[1 : length + 1] + taps[2] * padded[2:]
    )
    conv_y = (gate_b * convolved).astype(bf16)

    query_nope = attn_in[:, :edge_rot].astype(bf16)
    query_rot = jnp.concatenate(
        [
            rotate(attn_in[:, begin : begin + ROPE], cosine, sine)
            for begin in range(edge_rot, edge_lat, ROPE)
        ],
        axis=1,
    ).astype(bf16)

    final = None
    earlier = []
    for distance in [*range(count_sp - 1, 0, -1), 0]:
        target = (sp_index + distance) % count_sp
        if len(earlier) > 1:
            target = after(target, earlier[-2])
        keep, give = mix_block(
            target,
            tp_index,
            tok_rows,
            query_nope,
            query_rot,
            latent,
            key_rot,
            key_up,
            value_up,
            gain,
            conv_y,
            out_weight,
        )
        both = keep.astype(f32) + swapped(give, "tp", 1).astype(f32)
        if distance:
            both = both.astype(bf16)
            earlier.append(both)
            both = turned(both, "sp", distance).astype(f32)
        final = both if final is None else final + both
    return final.astype(bf16)[None]


def solution(mesh):
    sizes = dict(mesh.shape)
    divided = sizes["sp"] * sizes["tp"]
    fits = sizes["tp"] == 2 and sizes["fs"] == 4

    def shards(*args):
        heads = args[6].shape[1] // NOPE
        chans = args[2].shape[1]
        even = heads % sizes["sp"] == 0 and chans % sizes["sp"] == 0 and KVL % divided == 0
        even = even and sizes["sp"] % 2 == 0 and chans // sizes["sp"] % 128 == 0
        even = even and chans // sizes["sp"] == args[6].shape[0]
        if fits and even:
            return head_parallel(*args)
        return token_parallel(*args)

    return jax.shard_map(
        shards,
        mesh=mesh,
        in_specs=(
            P("fs", "sp", "tp"),
            P(),
            P(("sp", "fs"), "tp"),
            P(("sp", "fs"), "tp"),
            P(("sp", "fs"), "tp"),
            P(None, "tp"),
            P(("sp", "fs"), "tp"),
            P(("sp", "fs"), "tp"),
            P(("sp", "fs"), None),
            P(),
            P(),
            P(None, "tp"),
            P(None, "tp"),
            P("tp"),
            P("tp", ("sp", "fs")),
            P("tp", ("sp", "fs")),
        ),
        out_specs=P("fs", ("sp", "tp"), None),
        check_vma=False,
    )
```

```python
import jax
import jax.numpy as jnp
from jax import lax
from jax.experimental import pallas as pl
from jax.experimental.pallas import tpu as pltpu
from jax.sharding import PartitionSpec as P

NOPE = 128
ROPE = 64
VD = 128
KVL = 512
SEG = 64


norm_epsilon = 1e-06
rope_theta = 10000.0


def passed_along(block, axis, distance):
    devices = range(lax.axis_size(axis))
    route = [(i - distance, i) for i in devices if i - distance in devices]
    return lax.ppermute(block, axis, route)


def rms_scale(values, gain):
    return (
        values * lax.rsqrt(jnp.mean(values * values, axis=-1, keepdims=True) + norm_epsilon) * gain
    )


def rope_tables(positions):
    half_width = ROPE // 2
    frequency = rope_theta ** (-jnp.arange(half_width, dtype=jnp.float32) * 2.0 / ROPE)
    angles = positions[:, None] * frequency[None, :]
    return (jnp.cos(angles), jnp.sin(angles))


def rotate(values, cosine, sine):
    half_width = ROPE // 2
    first = values[..., :half_width]
    second = values[..., half_width:]
    return jnp.concatenate(
        [first * cosine - second * sine, second * cosine + first * sine], axis=-1
    )


def token_parallel(
    tokens,
    mix_gain,
    conv_b_weight,
    conv_c_weight,
    conv_v_weight,
    conv_taps,
    query_weight,
    query_rope_weight,
    latent_weight,
    key_rope_weight,
    latent_gain,
    key_up_weight,
    value_up_weight,
    head_gain,
    conv_out_weight,
    attn_out_weight,
):
    full_rows = lax.all_gather(tokens[0], "tp", axis=1, tiled=True)
    tok_rows = full_rows.shape[0]
    normed = rms_scale(full_rows.astype(jnp.float32), mix_gain).astype(jnp.bfloat16)
    offset = lax.axis_index("sp") * tok_rows
    token_index = offset + jnp.arange(tok_rows, dtype=jnp.int32)
    cosine, sine = rope_tables(token_index.astype(jnp.float32))
    local_heads = query_weight.shape[1] // NOPE
    count_sp = lax.axis_size("sp")
    count_fs = lax.axis_size("fs")
    count_tp = lax.axis_size("tp")
    fs_index = lax.axis_index("fs")
    row_piece = normed.shape[1] // (count_sp * count_fs)
    all_normed = lax.all_gather(normed, "fs", axis=0, tiled=True)
    picked = lax.dynamic_index_in_dim(
        all_normed.reshape(-1, count_sp, count_fs, row_piece), fs_index, 2, keepdims=False
    ).reshape(-1, count_sp * row_piece)
    gathered = (
        lax.all_gather(conv_b_weight, "sp", axis=0, tiled=True),
        lax.all_gather(conv_c_weight, "sp", axis=0, tiled=True),
        lax.all_gather(conv_v_weight, "sp", axis=0, tiled=True),
        lax.all_gather(query_weight, "sp", axis=0, tiled=True),
        lax.all_gather(query_rope_weight, "sp", axis=0, tiled=True),
        lax.all_gather(latent_weight, "sp", axis=0, tiled=True),
    )

    def project_in():
        return jnp.concatenate(
            [jnp.dot(picked, member, preferred_element_type=jnp.float32) for member in gathered],
            axis=1,
        )

    joined = lax.psum_scatter(
        project_in().astype(jnp.bfloat16), "fs", scatter_dimension=0, tiled=True
    ).astype(jnp.float32)
    bounds = []
    running_total = 0
    for member in gathered[:-1]:
        running_total = running_total + member.shape[1]
        bounds.append(running_total)
    sums = tuple(jnp.split(joined, bounds, axis=1))
    latent_raw = sums[5].astype(jnp.bfloat16)
    gate_b = sums[0].astype(jnp.bfloat16)
    gate_c = sums[1].astype(jnp.bfloat16)
    values_v = sums[2].astype(jnp.bfloat16)
    query_nope = sums[3].astype(jnp.bfloat16).reshape(tok_rows, local_heads, NOPE)
    query_rot = rotate(
        sums[4].reshape(tok_rows, local_heads, ROPE), cosine[:, None, :], sine[:, None, :]
    ).astype(jnp.bfloat16)
    latent = rms_scale(latent_raw.astype(jnp.float32), latent_gain).astype(jnp.bfloat16)
    key_rot = rotate(
        jnp.dot(normed, key_rope_weight, preferred_element_type=jnp.float32), cosine, sine
    ).astype(jnp.bfloat16)
    query_latent = jnp.einsum(
        "thn,khn->thk",
        query_nope,
        key_up_weight.reshape(KVL, local_heads, NOPE),
        preferred_element_type=jnp.float32,
    ).astype(jnp.bfloat16)
    attn_scale = (NOPE + ROPE) ** (-0.5)
    product = (gate_c.astype(jnp.float32) * values_v.astype(jnp.float32)).astype(jnp.bfloat16)
    previous = passed_along(product[tok_rows - 2 :], "sp", 1)
    padded = jnp.concatenate([previous, product], axis=0).astype(jnp.float32)
    convolved = (
        conv_taps[0] * padded[0:tok_rows]
        + conv_taps[1] * padded[1 : tok_rows + 1]
        + conv_taps[2] * padded[2 : tok_rows + 2]
    )
    conv_y = (gate_b.astype(jnp.float32) * convolved).astype(jnp.bfloat16)
    query_segment = token_index // SEG
    last_segment = (offset + tok_rows - 1) // SEG

    def key_block(running, latent_block, rot_block, first_key):
        peak_old, denom_old, accum_old = running
        block_rows = latent_block.shape[0]
        scores = (
            jnp.einsum(
                "thk,jk->thj", query_latent, latent_block, preferred_element_type=jnp.float32
            )
            + jnp.einsum("thr,jr->thj", query_rot, rot_block, preferred_element_type=jnp.float32)
        ) * attn_scale
        key_segment = (first_key + jnp.arange(block_rows, dtype=jnp.int32)) // SEG
        allowed = key_segment[None, None, :] <= query_segment[:, None, None]
        peak_new = jnp.maximum(peak_old, jnp.max(jnp.where(allowed, scores, -1e30), axis=-1))
        weights = jnp.where(allowed, jnp.exp(scores - peak_new[..., None]), 0.0)
        rescale = jnp.exp(peak_old - peak_new)
        denom_new = denom_old * rescale + jnp.sum(weights, axis=-1)
        accum_new = accum_old * rescale[..., None] + jnp.einsum(
            "thj,jk->thk",
            weights.astype(jnp.bfloat16),
            latent_block,
            preferred_element_type=jnp.float32,
        )
        return (peak_new, denom_new, accum_new)

    starting = (
        jnp.full((tok_rows, local_heads), -1e30, jnp.float32),
        jnp.zeros((tok_rows, local_heads), jnp.float32),
        jnp.zeros((tok_rows, local_heads, KVL), jnp.float32),
    )
    latent_piece = lax.all_gather(latent, "sp", axis=0, tiled=True)
    rot_piece = lax.all_gather(key_rot, "sp", axis=0, tiled=True)
    piece_rows = latent_piece.shape[0]
    splits = max(1, piece_rows // 512)
    while piece_rows % splits:
        splits = splits - 1
    block_rows = piece_rows // splits

    def visit(state, block_index):
        block_begin = block_index * block_rows
        latent_block = lax.dynamic_slice_in_dim(latent_piece, block_begin, block_rows, 0)
        rot_block = lax.dynamic_slice_in_dim(rot_piece, block_begin, block_rows, 0)
        updated = lax.cond(
            block_begin // SEG <= last_segment,
            lambda inner: key_block(inner, latent_block, rot_block, block_begin),
            lambda inner: inner,
            state,
        )
        return (updated, None)

    peak, denom, accum = lax.scan(visit, starting, jnp.arange(splits, dtype=jnp.int32))[0]
    attended = (accum / denom[..., None]).astype(jnp.bfloat16)
    head_out = jnp.einsum(
        "thk,khv->thv",
        attended,
        value_up_weight.reshape(KVL, local_heads, VD),
        preferred_element_type=jnp.float32,
    )
    normed_heads = rms_scale(head_out, head_gain.reshape(local_heads, VD))
    attn_y = normed_heads.astype(jnp.bfloat16).reshape(tok_rows, local_heads * VD)
    share_rows = tok_rows // count_tp
    conv_all, attn_all = (
        lax.all_gather(conv_y, "fs", axis=0, tiled=True),
        lax.all_gather(attn_y, "fs", axis=0, tiled=True),
    )
    conv_sorted = (
        conv_all.reshape(count_fs, count_tp, share_rows, -1)
        .transpose(1, 0, 2, 3)
        .reshape(count_fs * tok_rows, -1)
    )
    attn_sorted = (
        attn_all.reshape(count_fs, count_tp, share_rows, -1)
        .transpose(1, 0, 2, 3)
        .reshape(count_fs * tok_rows, -1)
    )
    conv_cols_sp, attn_cols_sp = (
        lax.all_gather(conv_out_weight, "sp", axis=1, tiled=True),
        lax.all_gather(attn_out_weight, "sp", axis=1, tiled=True),
    )
    col_sums = lax.psum_scatter(
        (
            jnp.dot(conv_sorted, conv_cols_sp, preferred_element_type=jnp.float32)
            + jnp.dot(attn_sorted, attn_cols_sp, preferred_element_type=jnp.float32)
        ).astype(jnp.bfloat16),
        "tp",
        scatter_dimension=0,
        tiled=True,
    )
    col_piece = conv_cols_sp.shape[1] // count_sp
    outgoing = col_sums.reshape(count_fs, share_rows, count_sp * col_piece)
    arrived = lax.all_to_all(outgoing, "fs", split_axis=0, concat_axis=2, tiled=True)
    result = (
        arrived.reshape(share_rows, count_fs, count_sp, col_piece)
        .transpose(0, 2, 1, 3)
        .reshape(share_rows, count_fs * count_sp * col_piece)
    )
    return result[None]


def turned(block, axis, distance):
    count = lax.axis_size(axis)
    return lax.ppermute(block, axis, [(i, (i + distance) % count) for i in range(count)])


def swapped(block, axis, mask):
    return lax.ppermute(block, axis, [(i, i ^ mask) for i in range(lax.axis_size(axis))])


def after(values, *others):
    return lax.optimization_barrier((values,) + others)[0]


def exchange(blocks, axis):
    return [blocks[0]] + [turned(blocks[d], axis, d) for d in range(1, len(blocks))]


def spread(block):
    by_one = swapped(block, "fs", 1)
    by_two = swapped(block, "fs", 2)
    half = block.shape[0] // 2
    upper = swapped(by_one[:half], "fs", 2)
    lower = swapped(by_two[half:], "fs", 1)
    return [[block], [by_one], [by_two], [upper, lower]]


def in_vmem(count):
    return [pl.BlockSpec(memory_space=pltpu.VMEM) for _ in range(count)]


def local_kernel(body, outs, scalars, *arrays):
    return pl.pallas_call(
        body,
        in_specs=[pl.BlockSpec(memory_space=pltpu.SMEM)] + in_vmem(len(arrays)),
        out_specs=in_vmem(len(outs)),
        out_shape=[jax.ShapeDtypeStruct(shape, jnp.bfloat16) for shape in outs],
    )(scalars, *arrays)


def pack_columns(index, count, groups, stacked):
    flat = [w for group in groups for w in group]
    rows = flat[0].shape[0]
    widths = [[w.shape[1] // count for w in group] for group in groups]
    stacks = [(w.shape[0] // count // rows, w.shape[1]) for w in stacked]
    tail = sum(pieces * width for pieces, width in stacks)
    full = [sum(group) for group in widths]
    full[-1] += tail
    outs = [(rows, full[g]) for g in range(len(groups)) for _ in range(count)]
    inputs = len(flat) + len(stacked)
    targets = (index + jnp.arange(count, dtype=jnp.int32)) % count

    def body(target_ref, *refs):
        ins, out_refs = refs[:inputs], refs[inputs:]
        taken = 0
        for g, group in enumerate(groups):
            for d in range(count):
                out = out_refs[g * count + d]
                begin = 0
                for i, width in enumerate(widths[g]):
                    source = pl.multiple_of(target_ref[d] * width, width)
                    out[:, begin : begin + width] = ins[taken + i][:, pl.ds(source, width)]
                    begin += width
            taken += len(group)
        for d in range(count):
            out = out_refs[(len(groups) - 1) * count + d]
            begin = sum(widths[-1])
            for i, (pieces, width) in enumerate(stacks):
                for j in range(pieces):
                    source = pl.multiple_of((target_ref[d] * pieces + j) * rows, rows)
                    out[:, begin : begin + width] = ins[len(flat) + i][pl.ds(source, rows), :]
                    begin += width

    made = local_kernel(body, outs, targets, *flat, *stacked)
    return [made[g * count : (g + 1) * count] for g in range(len(groups))]


def norm_columns(halves, others, gain, key_rope, tp_index, sp_index, order):
    count = len(halves)
    rows, half = halves[0].shape
    pieces = order.shape[0]
    width = 2 * half // pieces
    per_half = pieces // 2
    scalars = jnp.concatenate(
        [
            order,
            (sp_index - jnp.arange(count, dtype=jnp.int32)) % count,
            tp_index[None].astype(jnp.int32),
        ]
    )

    def body(scalar_ref, gain_ref, rope_ref, *refs):
        ins, (out, rope_out) = refs[: 2 * count], refs[2 * count :]
        side = scalar_ref[pieces + count]
        for d in range(count):
            mine, other = ins[d], ins[count + d]
            row = pl.multiple_of(scalar_ref[pieces + d] * rows, rows)
            square = jnp.zeros((rows, 1), jnp.float32)
            for ref in (mine, other):
                values = ref[...].astype(jnp.float32)
                square += jnp.sum(values * values, axis=1, keepdims=True)
            scale = lax.rsqrt(square / (2 * half) + norm_epsilon)
            for j in range(pieces):
                piece = scalar_ref[j]
                column = pl.multiple_of((piece % per_half) * width, width)
                local = mine[:, pl.ds(column, width)].astype(jnp.float32)
                far = other[:, pl.ds(column, width)].astype(jnp.float32)
                values = jnp.where(piece // per_half == side, local, far)
                factor = gain_ref[:, pl.ds(pl.multiple_of(piece * width, width), width)]
                out[pl.ds(row, rows), j * width : (j + 1) * width] = (
                    values * scale * factor
                ).astype(jnp.bfloat16)
        for j in range(pieces):
            begin = pl.multiple_of(scalar_ref[j] * width, width)
            rope_out[j * width : (j + 1) * width, :] = rope_ref[pl.ds(begin, width), :]

    outs = [(count * rows, 2 * half), key_rope.shape]
    return local_kernel(body, outs, scalars, gain[None, :], key_rope, *halves, *others)


def place_columns(parts, order, begin, rows, width):
    pieces = (parts[0].shape[1] - begin) // width
    places = order.shape[0]

    def body(order_ref, *refs):
        out = refs[-1]
        place = 0
        for ref in refs[:-1]:
            for top in range(0, ref.shape[0], rows):
                column = pl.multiple_of(order_ref[place] * width, width)
                for j in range(pieces):
                    left = begin + j * width
                    out[j * rows : (j + 1) * rows, pl.ds(column, width)] = ref[
                        top : top + rows, left : left + width
                    ]
                place += 1

    return local_kernel(body, [(pieces * rows, places * width)], order, *parts)[0]


def mix_block(target, tp_index, rows, query, query_rot, latent, key_rot, key_up, value_up, gain, conv_y, out_weight):
    heads = query.shape[1] // NOPE
    length = latent.shape[0]
    chans = conv_y.shape[1]
    columns = out_weight.shape[1]
    attn_scale = (NOPE + ROPE) ** (-0.5)
    transposed = (((1,), (1,)), ((), ()))

    def dot(left, right, dims=(((1,), (0,)), ((), ()))):
        return lax.dot_general(left, right, dims, preferred_element_type=jnp.float32)

    def body(s_ref, q_ref, qr_ref, lat_ref, kr_ref, ku_ref, vu_ref, g_ref, c_ref, w_ref, keep_ref, give_ref):
        row = pl.multiple_of(s_ref[0] * rows, rows)
        latents = lat_ref[...]
        keys_rot = kr_ref[...]
        own = (row + lax.broadcasted_iota(jnp.int32, (rows, length), 0)) // SEG
        theirs = lax.broadcasted_iota(jnp.int32, (rows, length), 1) // SEG
        allowed = theirs <= own
        mixed = dot(c_ref[pl.ds(row, rows), :], w_ref[:chans, :])
        for h in range(heads):
            low = dot(
                q_ref[pl.ds(row, rows), h * NOPE : (h + 1) * NOPE],
                ku_ref[:, h * NOPE : (h + 1) * NOPE],
                transposed,
            ).astype(jnp.bfloat16)
            rot = qr_ref[pl.ds(row, rows), h * ROPE : (h + 1) * ROPE]
            scores = (dot(low, latents, transposed) + dot(rot, keys_rot, transposed)) * attn_scale
            scores = jnp.where(allowed, scores, -1e30)
            top = jnp.max(scores, axis=-1, keepdims=True)
            weights = jnp.where(allowed, jnp.exp(scores - top), 0.0)
            total = jnp.sum(weights, axis=-1, keepdims=True)
            attended = (dot(weights.astype(jnp.bfloat16), latents) / total).astype(jnp.bfloat16)
            head_out = dot(attended, vu_ref[:, h * VD : (h + 1) * VD])
            attn_y = rms_scale(head_out, g_ref[:, h * VD : (h + 1) * VD]).astype(jnp.bfloat16)
            begin = chans + h * VD
            mixed += dot(attn_y, w_ref[begin : begin + VD, :])
        low_half = mixed[: rows // 2].astype(jnp.bfloat16)
        high_half = mixed[rows // 2 :].astype(jnp.bfloat16)
        first = s_ref[1] == 0
        keep_ref[...] = jnp.where(first, low_half, high_half)
        give_ref[...] = jnp.where(first, high_half, low_half)

    flops = 2 * rows * (
        heads * (length * (2 * KVL + ROPE) + KVL * (NOPE + VD)) + out_weight.shape[0] * columns
    )
    operands = (query, query_rot, latent, key_rot, key_up, value_up, gain[None, :], conv_y, out_weight)
    return pl.pallas_call(
        body,
        in_specs=[pl.BlockSpec(memory_space=pltpu.SMEM)] + in_vmem(len(operands)),
        out_specs=in_vmem(2),
        out_shape=[jax.ShapeDtypeStruct((rows // 2, columns), jnp.bfloat16)] * 2,
        cost_estimate=pl.CostEstimate(
            flops=flops, bytes_accessed=8 * rows * columns, transcendentals=heads * rows * length
        ),
    )(jnp.stack([target, tp_index]).astype(jnp.int32), *operands)


def head_parallel(
    tokens,
    mix_gain,
    conv_b_weight,
    conv_c_weight,
    conv_v_weight,
    conv_taps,
    query_weight,
    query_rope_weight,
    latent_weight,
    key_rope_weight,
    latent_gain,
    key_up_weight,
    value_up_weight,
    head_gain,
    conv_out_weight,
    attn_out_weight,
):
    count_sp = lax.axis_size("sp")
    count_fs = lax.axis_size("fs")
    count_tp = lax.axis_size("tp")
    sp_index = lax.axis_index("sp")
    fs_index = lax.axis_index("fs")
    tp_index = lax.axis_index("tp")
    bf16 = jnp.bfloat16
    f32 = jnp.float32
    tok_rows = tokens.shape[1]
    length = tok_rows * count_sp
    row_piece = query_weight.shape[0]
    heads = query_weight.shape[1] // NOPE // count_sp
    chans = conv_b_weight.shape[1] // count_sp
    lat_cols = latent_weight.shape[1] // count_sp
    sources = (sp_index - jnp.arange(count_sp, dtype=jnp.int32)) % count_sp
    faces = fs_index ^ jnp.arange(count_fs, dtype=jnp.int32)
    order = (sources[None, :] * count_fs + faces[:, None]).reshape(-1)

    pack_attn, pack_conv = pack_columns(
        sp_index,
        count_sp,
        (
            (query_weight, query_rope_weight, latent_weight),
            (conv_b_weight, conv_c_weight, conv_v_weight),
        ),
        (conv_out_weight, attn_out_weight),
    )
    arrived_attn = exchange(pack_attn, "sp")
    parts_attn = spread(jnp.concatenate(arrived_attn, axis=0))

    pack_conv = [after(block, *arrived_attn) for block in pack_conv]
    arrived_conv = exchange(pack_conv, "sp")
    joined_conv = jnp.concatenate(arrived_conv, axis=0)
    pieces_attn = [p for part in parts_attn for p in part]
    parts_conv = spread(after(joined_conv, *pieces_attn))

    own = tokens[0]
    sent = after(own, *arrived_conv)
    halves = [own] + [turned(sent, "sp", d) for d in range(1, count_sp)]
    others = [swapped(half, "tp", 1) for half in halves]
    norm_gain = after(mix_gain, parts_conv[1][0], parts_conv[2][0])
    normed, key_rope = norm_columns(
        halves, others, norm_gain, key_rope_weight, tp_index, sp_index, order
    )

    def project(parts, width):
        total = 0.0
        begin = 0
        for part in parts:
            for piece in part:
                columns = normed[:, begin : begin + piece.shape[0]]
                total = total + jnp.dot(columns, piece[:, :width], preferred_element_type=f32)
                begin += piece.shape[0]
        return total

    attn_in = project(parts_attn, parts_attn[0][0].shape[1])
    edge_rot = heads * NOPE
    edge_lat = edge_rot + heads * ROPE
    lat_rows = length // count_tp
    lat_own = lax.dynamic_slice_in_dim(
        attn_in[:, edge_lat:].astype(bf16), tp_index * lat_rows, lat_rows, 0
    )
    lat_blocks = [lat_own] + [turned(lat_own, "sp", d) for d in range(1, count_sp)]
    lat_mine = jnp.concatenate(lat_blocks, axis=1)
    lat_other = swapped(lat_mine, "tp", 1)
    latent_raw = jnp.where(
        tp_index == 0,
        jnp.concatenate([lat_mine, lat_other], axis=0),
        jnp.concatenate([lat_other, lat_mine], axis=0),
    )

    def turned_rows(weight, width, begin):
        return jnp.concatenate(
            [
                lax.dynamic_slice(weight, (sources[d] * lat_cols, begin), (lat_cols, width))
                for d in range(count_sp)
            ],
            axis=0,
        )

    lat_gain = turned_rows(latent_gain[:, None], 1, 0)[:, 0]
    latent = rms_scale(latent_raw.astype(f32), lat_gain).astype(bf16)

    position = jnp.arange(length, dtype=jnp.int32)
    cosine, sine = rope_tables(position.astype(f32))
    key_rot = rotate(
        jnp.dot(normed, key_rope, preferred_element_type=f32), cosine, sine
    ).astype(bf16)

    key_up = turned_rows(key_up_weight, heads * NOPE, sp_index * heads * NOPE)
    value_up = turned_rows(value_up_weight, heads * VD, sp_index * heads * VD)
    gain = lax.dynamic_slice_in_dim(head_gain, sp_index * heads * VD, heads * VD, 0)
    taps = lax.dynamic_slice_in_dim(conv_taps, sp_index * chans, chans, 1)

    pieces_conv = [p for part in parts_conv for p in part]
    out_weight = place_columns(
        pieces_conv, order, 3 * chans, row_piece, conv_out_weight.shape[1]
    )

    conv_in = project(parts_conv, 3 * chans).astype(bf16).astype(f32)
    gate_b = conv_in[:, :chans]
    product = (conv_in[:, chans : 2 * chans] * conv_in[:, 2 * chans :]).astype(bf16)
    padded = jnp.concatenate([jnp.zeros((2, chans), bf16), product], axis=0).astype(f32)
    convolved = (
        taps[0] * padded[0:length] + taps[1] * padded[1 : length + 1] + taps[2] * padded[2:]
    )
    conv_y = (gate_b * convolved).astype(bf16)

    query_nope = attn_in[:, :edge_rot].astype(bf16)
    query_rot = jnp.concatenate(
        [
            rotate(attn_in[:, begin : begin + ROPE], cosine, sine)
            for begin in range(edge_rot, edge_lat, ROPE)
        ],
        axis=1,
    ).astype(bf16)

    final = None
    earlier = []
    for distance in [*range(count_sp - 1, 0, -1), 0]:
        target = (sp_index + distance) % count_sp
        if len(earlier) > 1:
            target = after(target, earlier[-2])
        keep, give = mix_block(
            target,
            tp_index,
            tok_rows,
            query_nope,
            query_rot,
            latent,
            key_rot,
            key_up,
            value_up,
            gain,
            conv_y,
            out_weight,
        )
        both = keep.astype(f32) + swapped(give, "tp", 1).astype(f32)
        if distance:
            both = both.astype(bf16)
            earlier.append(both)
            both = turned(both, "sp", distance).astype(f32)
        final = both if final is None else final + both
    return final.astype(bf16)[None]


def solution(mesh):
    sizes = dict(mesh.shape)
    divided = sizes["sp"] * sizes["tp"]
    fits = sizes["tp"] == 2 and sizes["fs"] == 4

    def shards(*args):
        heads = args[6].shape[1] // NOPE
        chans = args[2].shape[1]
        even = heads % sizes["sp"] == 0 and chans % sizes["sp"] == 0 and KVL % divided == 0
        even = even and sizes["sp"] % 2 == 0 and chans // sizes["sp"] % 128 == 0
        even = even and chans // sizes["sp"] == args[6].shape[0]
        if fits and even:
            return head_parallel(*args)
        return token_parallel(*args)

    return jax.shard_map(
        shards,
        mesh=mesh,
        in_specs=(
            P("fs", "sp", "tp"),
            P(),
            P(("sp", "fs"), "tp"),
            P(("sp", "fs"), "tp"),
            P(("sp", "fs"), "tp"),
            P(None, "tp"),
            P(("sp", "fs"), "tp"),
            P(("sp", "fs"), "tp"),
            P(("sp", "fs"), None),
            P(),
            P(),
            P(None, "tp"),
            P(None, "tp"),
            P("tp"),
            P("tp", ("sp", "fs")),
            P("tp", ("sp", "fs")),
        ),
        out_specs=P("fs", ("sp", "tp"), None),
        check_vma=False,
    )
```
